32 devices in a mesh: ep: 8 (over z, y), tp: 4 (over x, core).
Axes of the slice: x: 2, y: 2, z: 4, core: 2. Of those that a mesh axis runs over, the one named last changes fastest.
Arguments:
- x_mix: bfloat16 [8192, 2048], P('ep'), may hold values from -6 to 6
- mix_gain: float32 [2048], replicated, may hold values from 0.1 to 1.9
- w_query: bfloat16 [2048, 1024], P(None, 'tp'), may hold values from -0.125 to 0.125
- w_key: bfloat16 [2048, 1024], P(None, 'tp'), may hold values from -0.125 to 0.125
- w_value: bfloat16 [2048, 1024], P(None, 'tp'), may hold values from -0.125 to 0.125
- w_outgate: bfloat16 [2048, 1024], P(None, 'tp'), may hold values from -0.125 to 0.125
- w_gates: bfloat16 [2048, 32], replicated, may hold values from -0.125 to 0.125
- gate_bias: float32 [4, 8], P(None, 'tp'), may hold values from -1 to 120, as said below
- gate_drift: float32 [32], P('ep'), may hold values from -1.5 to 1.5
- head_gain: float32 [1024], P('tp'), may hold values from 0.1 to 1.9
- w_out: bfloat16 [1024, 2048], P('tp'), may hold values from -0.1875 to 0.1875
- x_route: bfloat16 [4096, 2048], P('ep'), may hold values from -6 to 6
- route_gain: float32 [2048], replicated, may hold values from 0.1 to 1.9
- routes: int32 [4096, 2], P('ep'), may hold values from 0 to 7, all different within a row; in each aligned block of 128 rows (0 to 127, 128 to 255, ...) at most 64 rows name the same one
- route_weight: float32 [4096, 2], P(('ep', 'tp')), may hold values from 0.2 to 1
- w_gate_e: bfloat16 [8, 2048, 1024], P('ep', None, 'tp'), may hold values from -0.125 to 0.125
- w_up_e: bfloat16 [8, 2048, 1024], P('ep', None, 'tp'), may hold values from -0.125 to 0.125
- w_down_e: bfloat16 [8, 1024, 2048], P('ep', 'tp'), may hold values from -0.1875 to 0.1875
Outputs:
- mixer_out: bfloat16 [8192, 2048], P(('ep', 'tp'))
- route_out: bfloat16 [4096, 2048], P(('ep', 'tp'))
The draws below stay inside these ranges and needn't reach their ends.
Inputs may be any that keep to these rules, and one draw needn't show every extreme that they name: `routes`: in each aligned block of 128 rows, no expert is named by more than 64 entries; the 2 experts of a row differ. `gate_bias`: rows 0 and 2 are input gate offsets, rows 1 and 3 forget gate offsets.
All inputs are finite; a program needn't handle non-finite values.
Results may differ from the reference program's by a relative error of at most 0.017.
Values may be sent and summed in bfloat16 or wider, within the bound.
A program may use at most 128 MiB of HBM per device.

```python
import math
import jax
import jax.numpy as jnp
import numpy as np
from jax import lax

D = 2048
HM = 8
HD = 128
FE = 1024
TOPK = 2
BLK = 256
EXPERTS = 8
TOKENS_A = 8192
TOKENS_B = 4096
QROWS = 128
CAPQ = 64
N_TP = 4


def draw_gate_bias(key, part):
    subkeys = jax.random.split(jax.random.fold_in(key, 17), 4)
    inputs = jax.random.uniform(subkeys[0], (2, HM), jnp.float32, -1.0, 1.0)
    slow_heads = jax.random.bernoulli(subkeys[1], 0.5, (2, HM))
    fast_values = jax.random.uniform(subkeys[2], (2, HM), jnp.float32, 4.0, 5.0)
    slow_values = jax.random.uniform(subkeys[3], (2, HM), jnp.float32, 11.0, 12.5)
    forget = jnp.where(slow_heads, slow_values, fast_values)
    return jnp.stack([inputs[0], forget[0], inputs[1], forget[1]], axis=0)


def steps_of(own_key, shape, cuts, smallest, top_value):
    def one(dim, parts):
        steps = jax.random.uniform(jax.random.fold_in(jax.random.fold_in(own_key, 6), dim), (parts,), jnp.float32, smallest / len(cuts), top_value / len(cuts))
        return jnp.repeat(jnp.exp(steps), shape[dim] // parts).reshape((-1,) + (1,) * (len(shape) - dim - 1))

    level = one(*cuts[0])
    for cut in cuts[1:]:
        level = level * one(*cut)
    return level


def routed_block(rng, own, number, rows, count, top, bound, skew):
    order = jax.random.permutation(rng, count)
    crowded, usual = load_shares(count, rows * top, bound, skew, True), load_shares(count, rows * top, bound, skew, False)
    places = jnp.arange(count)

    def named(lengths, turn):
        used = int((lengths > 0).sum())
        fixed = max(1, used // 4)
        moved = fixed + (places - fixed + turn * (used - fixed)) % max(1, count - fixed)
        return jnp.zeros((count,), jnp.int32).at[order[jnp.where(places < fixed, places, moved)]].set(jnp.asarray(lengths, jnp.int32))

    lengths = jnp.where(number % 4 == 0, named(crowded, number // 4), named(usual, number - number // 4 - 1))
    mixed = jax.random.permutation(jax.random.fold_in(own, 3), count)
    donor, taker = mixed[0:count // 2 * 2:2], mixed[1:count // 2 * 2:2]
    margin = jnp.minimum(lengths[donor] - 1, bound - lengths[taker]) // 2
    margin = jnp.where((donor == order[0]) | (taker == order[0]) | (lengths[taker] == 0), 0, jnp.maximum(margin, 0))
    moved = jax.random.randint(jax.random.fold_in(own, 4), (count // 2,), 0, 1 << 20) % (margin + 1)
    lengths = lengths.at[donor].add(-moved).at[taker].add(moved)
    members = jnp.searchsorted(jnp.cumsum(lengths), jnp.arange(rows * top), side="right").astype(jnp.int32)
    table = members.reshape(top, rows).T
    table = table[jax.random.permutation(jax.random.fold_in(own, 1), rows)]
    turn = jax.random.randint(jax.random.fold_in(own, 2), (rows, 1), 0, top)
    return jnp.take_along_axis(table, (jnp.arange(top)[None, :] + turn) % top, axis=1)


def load_shares(amount, total, most, skew, full):
    weights = [(1 << 20) // math.isqrt(rank ** skew) + 1 for rank in range(1, amount + 1)]
    largest = most if full else min(most, max(-(-total // amount), total * weights[0] // sum(weights)))
    least = 1 if total - largest >= amount - 1 else 0
    given, surplus = [largest] + [least] * (amount - 1), total - largest - least * (amount - 1)
    while surplus > 0:
        movable = [i for i in range(1, amount) if given[i] < largest] or [i for i in range(1, amount) if given[i] < most]
        pool, remaining = sum([weights[i] for i in movable]), surplus
        for i in movable:
            extra = min(most - given[i], max(1, remaining * weights[i] // pool), surplus)
            given[i] = given[i] + extra
            surplus = surplus - extra
    return np.array(given)


def noise(own_key, dims, deviation, bound, cuts=(), kind=jnp.bfloat16):
    array = jax.random.normal(own_key, dims, jnp.float32) * deviation
    if len(cuts) > 0:
        array = steps_of(own_key, dims, cuts, -0.22, 0.18) * array
    return jnp.clip(array, min=-bound, max=bound).astype(kind)


def setup_inputs(seed: int = 0) -> dict:
    seeds = jax.random.split(jax.random.key(seed), 19)
    x_mix = noise(seeds[0], (TOKENS_A, D), 1.0, 6.0, ((0, 8),))
    mix_gain = jnp.clip(1.0 + 0.18 * jax.random.normal(seeds[1], (D,), jnp.float32), 0.1, 1.9)
    w_query = noise(seeds[2], (D, HM * HD), D ** -0.5, 0.125, ((1, 4),))
    w_key = noise(seeds[3], (D, HM * HD), D ** -0.5, 0.125, ((1, 4),))
    w_value = noise(seeds[4], (D, HM * HD), D ** -0.5, 0.125, ((1, 4),))
    w_outgate = noise(seeds[5], (D, HM * HD), D ** -0.5, 0.125, ((1, 4),))
    w_gates = noise(seeds[6], (D, 4 * HM), D ** -0.5, 0.125)
    gate_bias = draw_gate_bias(jax.random.fold_in(seeds[18], 71), 0)
    gate_drift = jnp.clip(jax.random.uniform(seeds[8], (TOKENS_A // BLK,), jnp.float32, -1.5, 1.5) * steps_of(seeds[8], (TOKENS_A // BLK,), ((0, 8),), -0.4, 0.0), -1.5, 1.5)
    head_gain = jnp.clip(1.0 + 0.18 * jax.random.normal(seeds[9], (HM * HD,), jnp.float32), 0.1, 1.9)
    w_out = noise(seeds[10], (HM * HD, D), (HM * HD) ** -0.5, 0.1875, ((0, 4),))
    x_route = noise(seeds[11], (TOKENS_B, D), 1.0, 6.0, ((0, 8),))
    route_gain = jnp.clip(1.0 + 0.18 * jax.random.normal(seeds[12], (D,), jnp.float32), 0.1, 1.9)
    routes_keys = jax.random.split(jax.random.fold_in(seeds[13], 1), TOKENS_B // QROWS)
    routes_turns = jax.random.permutation(jax.random.fold_in(seeds[13], 3), TOKENS_B // QROWS)
    routes = jax.vmap(lambda own, number: routed_block(jax.random.fold_in(seeds[13], 2), own, number, QROWS, EXPERTS, TOPK, CAPQ, 2))(routes_keys, routes_turns).reshape((TOKENS_B, TOPK))
    route_weight = jnp.clip(0.2 + 0.8 * jax.random.uniform(seeds[14], (TOKENS_B, TOPK), jnp.float32) ** steps_of(seeds[14], (TOKENS_B, TOPK), ((0, 32),), -0.2, 0.2), 0.2, 1.0)
    w_gate_e = noise(seeds[15], (EXPERTS, D, FE), D ** -0.5, 0.125, ((0, 8), (2, 4)))
    w_up_e = noise(seeds[16], (EXPERTS, D, FE), D ** -0.5, 0.125, ((0, 8), (2, 4)))
    w_down_e = noise(seeds[17], (EXPERTS, FE, D), FE ** -0.5, 0.1875, ((0, 8), (1, 4)))
    return {"x_mix": x_mix, "mix_gain": mix_gain, "w_query": w_query, "w_key": w_key, "w_value": w_value, "w_outgate": w_outgate, "w_gates": w_gates, "gate_bias": gate_bias, "gate_drift": gate_drift, "head_gain": head_gain, "w_out": w_out, "x_route": x_route, "route_gain": route_gain, "routes": routes, "route_weight": route_weight, "w_gate_e": w_gate_e, "w_up_e": w_up_e, "w_down_e": w_down_e}


EPS = 1e-06
NEG = -1e+30
HIGH = lax.Precision.HIGHEST

def rms_scale(tensor, gain):
    tensor = tensor.astype(jnp.float32)
    return tensor * lax.rsqrt(lax.optimization_barrier(jnp.mean(tensor * tensor, axis=-1, keepdims=True)) + EPS) * gain.astype(jnp.float32)

def run_blocks(query, key_rows, value_rows, log_input, log_forget, state_in):
    head_count, row_count, head_width = query.shape
    block_count = row_count // BLK

    def in_blocks(tensor):
        return jnp.moveaxis(tensor.reshape((head_count, block_count, BLK) + tensor.shape[2:]), 1, 0)
    tri_mask = jnp.tril(jnp.ones((BLK, BLK), dtype=bool))

    def advance(state_now, pieces):
        memory, normer, stable = state_now
        q_block, k_block, v_block, in_block, forget_block = pieces
        q_wide = q_block.astype(jnp.float32)
        k_wide = k_block.astype(jnp.float32)
        v_wide = v_block.astype(jnp.float32)
        running = jnp.cumsum(forget_block, axis=-1)
        log_decay = jnp.where(tri_mask, running[:, :, None] - running[:, None, :] + in_block[:, None, :], NEG)
        carried = running + stable[:, None]
        stable_t = jnp.maximum(carried, lax.optimization_barrier(jnp.max(log_decay, axis=-1)))
        raw = jnp.einsum('htd,hsd->hts', q_block, k_block, preferred_element_type=jnp.float32)
        scores = raw * jnp.exp(log_decay - stable_t[:, :, None])
        carried_w = jnp.exp(carried - stable_t)
        numerator = jnp.einsum('hts,hse->hte', scores, v_wide, precision=HIGH) + carried_w[:, :, None] * jnp.einsum('htd,hde->hte', q_wide, memory, precision=HIGH)
        denominator = lax.optimization_barrier(jnp.sum(scores, axis=-1)) + carried_w * jnp.einsum('htd,hd->ht', q_wide, normer, precision=HIGH)
        result = numerator / jnp.maximum(jnp.abs(denominator), jnp.exp(-stable_t))[:, :, None]
        block_total = running[:, -1]
        log_weight = block_total[:, None] - running + in_block
        stable_new = jnp.maximum(block_total + stable, lax.optimization_barrier(jnp.max(log_weight, axis=-1)))
        weights = jnp.exp(log_weight - stable_new[:, None])
        shrink = jnp.exp(block_total + stable - stable_new)
        memory = shrink[:, None, None] * memory + jnp.einsum('hs,hsd,hse->hde', weights, k_wide, v_wide, precision=HIGH)
        normer = shrink[:, None] * normer + jnp.einsum('hs,hsd->hd', weights, k_wide, precision=HIGH)
        return ((memory, normer, stable_new), result)
    final_state, outputs = lax.scan(advance, state_in, tuple((in_blocks(t) for t in (query, key_rows, value_rows, log_input, log_forget))))
    return jnp.moveaxis(outputs, 0, 1).reshape(head_count, row_count, head_width)

def reverse_rows(tensor):
    return jnp.flip(tensor, axis=1)

def group_sum(left, right, groups):
    part_size = left.shape[1] // groups
    total = jnp.zeros((left.shape[0], right.shape[1]), jnp.float32)
    for group in range(groups):
        piece = jnp.dot(left[:, group * part_size:(group + 1) * part_size], right[group * part_size:(group + 1) * part_size], preferred_element_type=jnp.float32)
        total = total + lax.optimization_barrier(piece.astype(jnp.bfloat16)).astype(jnp.float32)
    return total.astype(jnp.bfloat16)

def reference(x_mix, mix_gain, w_query, w_key, w_value, w_outgate, w_gates, gate_bias, gate_drift, head_gain, w_out, x_route, route_gain, routes, route_weight, w_gate_e, w_up_e, w_down_e):
    seq_len = x_mix.shape[0]
    normed = rms_scale(x_mix, mix_gain).astype(jnp.bfloat16)
    query = jnp.dot(normed, w_query, preferred_element_type=jnp.float32).astype(jnp.bfloat16)
    key_rows = (jnp.dot(normed, w_key, preferred_element_type=jnp.float32) * HD ** (-0.5)).astype(jnp.bfloat16)
    value_rows = jnp.dot(normed, w_value, preferred_element_type=jnp.float32).astype(jnp.bfloat16)
    outgate = jnp.dot(normed, w_outgate, preferred_element_type=jnp.float32).astype(jnp.bfloat16)
    gate_pre = jnp.dot(normed, w_gates, preferred_element_type=jnp.float32).reshape(seq_len, 4, HM) + gate_bias[None]
    drift = jnp.repeat(gate_drift, BLK)[:, None]
    in_fw = gate_pre[:, 0].T
    forget_fw = jax.nn.log_sigmoid(gate_pre[:, 1] + drift).T
    in_bw = gate_pre[:, 2].T
    forget_bw = jax.nn.log_sigmoid(gate_pre[:, 3] + drift).T

    def heads_first(tensor):
        return tensor.reshape(seq_len, HM, HD).transpose(1, 0, 2)

    def one_head(pieces):
        q_head, k_head, v_head, in_f, forget_f, in_b, forget_b = pieces
        start = (jnp.zeros((1, HD, HD), jnp.float32), jnp.zeros((1, HD), jnp.float32), jnp.zeros((1,), jnp.float32))
        forward = run_blocks(q_head[None], k_head[None], v_head[None], in_f[None], forget_f[None], start)
        backward = reverse_rows(run_blocks(reverse_rows(q_head[None]), reverse_rows(k_head[None]), reverse_rows(v_head[None]), reverse_rows(in_b[None]), reverse_rows(forget_b[None]), start))
        return (forward + backward)[0]
    mixed = lax.map(one_head, (heads_first(query), heads_first(key_rows), heads_first(value_rows), in_fw, forget_fw, in_bw, forget_bw))
    mixed = mixed.transpose(1, 0, 2)
    gated = jax.nn.sigmoid(outgate.astype(jnp.float32)).reshape(seq_len, HM, HD) * mixed
    head_rows = rms_scale(gated, head_gain.reshape(HM, HD)).astype(jnp.bfloat16).reshape(seq_len, HM * HD)
    mixer_out = group_sum(head_rows, w_out, N_TP)
    token_count = x_route.shape[0]
    route_normed = rms_scale(x_route, route_gain).astype(jnp.bfloat16)
    block_total = token_count // QROWS
    flat_routes = routes.reshape(block_total, QROWS * TOPK)
    onehot = (flat_routes[:, :, None] == jnp.arange(EXPERTS, dtype=jnp.int32)[None, None, :]).astype(jnp.int32)
    ranks = lax.optimization_barrier(jnp.sum((jnp.cumsum(onehot, axis=1) - onehot) * onehot, axis=2))
    per_expert = block_total * CAPQ
    slots = (flat_routes * per_expert + jnp.arange(block_total, dtype=jnp.int32)[:, None] * CAPQ + ranks).reshape(-1).astype(jnp.int32)
    token_ids = jnp.repeat(jnp.arange(token_count, dtype=jnp.int32), TOPK)
    table = jnp.full((EXPERTS * per_expert,), token_count, jnp.int32).at[slots].set(token_ids)
    padded = jnp.concatenate([route_normed, jnp.zeros((1, route_normed.shape[1]), route_normed.dtype)], axis=0)

    def expert(pieces):
        index, gate_w, up_w, down_w = pieces
        picked_rows = padded[index]
        gate_part = jnp.dot(picked_rows, gate_w, preferred_element_type=jnp.float32)
        up_part = jnp.dot(picked_rows, up_w, preferred_element_type=jnp.float32)
        hidden = (jax.nn.silu(gate_part) * up_part).astype(jnp.bfloat16)
        return group_sum(hidden, down_w, N_TP)
    results = lax.map(expert, (table.reshape(EXPERTS, per_expert), w_gate_e, w_up_e, w_down_e))
    chosen = results.reshape(EXPERTS * per_expert, -1)[slots].reshape(token_count, TOPK, -1).astype(jnp.float32)
    route_out = lax.optimization_barrier(jnp.sum(route_weight[:, :, None] * chosen, axis=1)).astype(jnp.bfloat16)
    return (mixer_out, route_out)
```

```python
import functools

import jax
import jax.numpy as jnp
from jax import lax
from jax.experimental import pallas as pl
from jax.experimental.pallas import tpu as pltpu
from jax.sharding import PartitionSpec as P

HD = 128
TOPK = 2
BLK = 256
EPS = 1e-06
NEG = -1e30
MESH = pl.DeviceIdType.MESH
F32 = jnp.float32
BF16 = jnp.bfloat16
LANES = 128
CHUNK = 512


def nn(a, b):
    return lax.dot_general(a, b, (((1,), (0,)), ((), ())), preferred_element_type=F32)


def nt(a, b):
    return lax.dot_general(a, b, (((1,), (1,)), ((), ())), preferred_element_type=F32)


def tn(a, b):
    return lax.dot_general(a, b, (((0,), (0,)), ((), ())), preferred_element_type=F32)


def rms(rows, gain):
    rows = rows.astype(F32)
    return rows * lax.rsqrt(jnp.mean(rows * rows, axis=-1, keepdims=True) + EPS) * gain


def body(
    E, TP, heads, cap, quarter,
    x_mix, wq, wk, wv, wo, x_route, wg_e, wu_e, wd_e, w_out,
    mix_gain, route_gain, head_gain, w_gates, gate_add, routes, weights,
    mixer_out, route_out,
    xm, wqv, wkv, wvv, wov, xr, wgv, wuv, wdv, wfull, wts,
    sendbuf, xin, yboth, yrecv, retsend, ret, outsend, outrecv,
    qs, ks, vs, os_, rowsv, colsv, abuf, kvb, nb, stsend, scsend, strecv, screcv,
    cin, nin, min_, hsend, hrecv, slot_v,
    lsem, own_sem, d_send, d_recv, f_send, f_recv, y_send, y_recv, r_send, r_recv,
    s_send, s_recv, c_send, c_recv, h_send, h_recv, w_send, w_recv, g_send, g_recv, o_send, o_recv,
):
    e = lax.axis_index("ep")
    t = lax.axis_index("tp")
    lo = lax.rem(t, 2)
    hi = lax.div(t, 2)
    mate = t + 1 - 2 * lo
    H = TP // 2
    R = H * cap
    D = xm.shape[1]
    NB = xm.shape[0] // BLK
    slots = E * cap

    loads = []
    for h in range(H):
        loads.append(pltpu.make_async_copy(
            x_route.at[pl.ds((2 * h + lo) * quarter, quarter)], xr.at[h], lsem.at[h]))
    for i, (src, dst) in enumerate([
        (x_mix, xm), (wq, wqv), (wk, wkv), (wv, wvv), (wo, wov),
        (wg_e, wgv), (wu_e, wuv), (wd_e, wdv), (w_out, wfull.at[t]),
    ]):
        loads.append(pltpu.make_async_copy(src, dst, lsem.at[H + i]))
    loads.append(pltpu.make_async_copy(weights, wts.at[hi], lsem.at[H + 9]))
    for c in loads:
        c.start()

    barrier = pltpu.get_barrier_semaphore()
    for k in range(1, E):
        pl.semaphore_signal(barrier, inc=1, device_id=(lax.rem(e + k, E), t), device_id_type=MESH)
    for k in range(1, TP):
        pl.semaphore_signal(barrier, inc=1, device_id=(e, lax.rem(t + k, TP)), device_id_type=MESH)
    pl.semaphore_wait(barrier, E - 1 + TP - 1)

    tri = (lax.broadcasted_iota(jnp.int32, (quarter, quarter), 0)
           > lax.broadcasted_iota(jnp.int32, (quarter, quarter), 1)).astype(BF16)
    for h in range(H):
        loads[h].wait()
        rows = rms(xr[h], route_gain[...]).astype(BF16)
        table = routes[pl.ds((2 * h + lo) * quarter, quarter), :]
        experts = lax.broadcasted_iota(jnp.int32, (quarter, E), 1)
        hot = [(experts == table[:, j:j + 1]).astype(F32) for j in range(TOPK)]
        before = nn(tri, sum(hot).astype(BF16))
        place = lax.broadcasted_iota(jnp.int32, (quarter, slots), 1)
        pick = None
        for j in range(TOPK):
            slot = table[:, j:j + 1] * cap + jnp.sum(before * hot[j], axis=1, keepdims=True).astype(jnp.int32)
            slot_v[h, j] = jnp.broadcast_to(slot, (quarter, LANES))
            here = (place == slot).astype(F32)
            pick = here if pick is None else pick + here
        pick = pick.astype(BF16)
        for c in range(0, D, CHUNK):
            packed = tn(pick, rows[:, c:c + CHUNK]).astype(BF16)
            sendbuf[:, h * cap:(h + 1) * cap, c:c + CHUNK] = packed.reshape(E, cap, CHUNK)

    def dispatch(k):
        to = lax.rem(e + k, E)
        return pltpu.make_async_remote_copy(
            src_ref=sendbuf.at[to], dst_ref=xin.at[lo, e], send_sem=d_send.at[k], recv_sem=d_recv.at[k],
            device_id=(to, t), device_id_type=MESH)

    own = pltpu.make_async_copy(sendbuf.at[e], xin.at[lo, e], own_sem.at[0])
    own.start()
    for k in range(1, E):
        dispatch(k).start()

    loads[H + 8].wait()
    loads[H + 9].wait()

    def share_w(k):
        return pltpu.make_async_remote_copy(
            src_ref=wfull.at[t], dst_ref=wfull.at[t], send_sem=w_send.at[k], recv_sem=w_recv.at[k],
            device_id=(e, lax.rem(t + k, TP)), device_id_type=MESH)

    def share_g(k):
        return pltpu.make_async_remote_copy(
            src_ref=wts.at[hi], dst_ref=wts.at[hi], send_sem=g_send.at[k], recv_sem=g_recv.at[k],
            device_id=(e, lax.rem(t + 2 * k, TP)), device_id_type=MESH)

    for k in range(1, H):
        share_g(k).start()
    for k in range(1, TP):
        share_w(k).start()

    for i in range(5):
        loads[H + i].wait()
    pos_r = lax.broadcasted_iota(jnp.int32, (BLK, BLK), 0)
    pos_c = lax.broadcasted_iota(jnp.int32, (BLK, BLK), 1)

    def project(j, carry):
        at = pl.ds(pl.multiple_of(j * BLK, BLK), BLK)
        normed = rms(xm[at, :], mix_gain[...]).astype(BF16)
        qs[at, :] = nn(normed, wqv[...]).astype(BF16)
        k_all = (nn(normed, wkv[...]) * (HD ** -0.5)).astype(BF16)
        v_all = nn(normed, wvv[...]).astype(BF16)
        ks[at, :] = k_all
        vs[at, :] = v_all
        os_[at, :] = nn(normed, wov[...]).astype(BF16)
        pre = nt(w_gates[...], normed) + gate_add[j]
        logf = jnp.minimum(pre, 0.0) - jnp.log1p(jnp.exp(-jnp.abs(pre)))
        upper = (pos_r <= pos_c).astype(F32)
        lower = (pos_r >= pos_c).astype(F32)
        cum = jnp.dot(logf, upper, precision=lax.Precision.HIGHEST, preferred_element_type=F32)
        rev = jnp.dot(logf, lower, precision=lax.Precision.HIGHEST, preferred_element_type=F32)
        b_fw = cum[heads:2 * heads]
        b_bw = rev[3 * heads:4 * heads]
        a_fw = pre[0:heads] - b_fw
        a_bw = pre[2 * heads:3 * heads] - b_bw
        rows = jnp.concatenate([a_fw, a_bw, b_fw, b_bw], axis=0)
        cols = jnp.transpose(rows)
        rowsv[j] = rows
        colsv[j] = cols
        scal = []
        for d in range(2):
            for h in range(heads):
                i = d * heads + h
                top = jnp.max(rows[i:i + 1], axis=1, keepdims=True)
                scal.append(jnp.broadcast_to(top, (1, LANES)))
                w_col = jnp.exp(cols[:, i:i + 1] - top)
                hs = slice(h * HD, (h + 1) * HD)
                kw = k_all[:, hs].astype(F32) * w_col
                kvb[j, i] = tn(kw.astype(BF16), v_all[:, hs])
                nb[j, i:i + 1] = jnp.sum(kw, axis=0, keepdims=True)
        for d in range(2):
            for h in range(heads):
                i = 2 * heads + d * heads + h
                end = rows[i:i + 1, BLK - 1:BLK] if d == 0 else rows[i:i + 1, 0:1]
                scal.append(jnp.broadcast_to(end, (1, LANES)))
        abuf[j] = jnp.concatenate(scal, axis=0)
        return carry

    lax.fori_loop(0, NB, project, 0)

    def advance(state, i, j):
        mem, nor, m = state
        top = abuf[j, i:i + 1]
        tot = abuf[j, 2 * heads + i:2 * heads + i + 1]
        g = jnp.maximum(m, top)
        old, new = jnp.exp(m - g), jnp.exp(top - g)
        return (old * mem + new * kvb[j, i], old * nor + new * nb[j, i:i + 1], tot + g)

    def order(d):
        return range(NB) if d == 0 else range(NB - 1, -1, -1)

    for d in range(2):
        for h in range(heads):
            i = d * heads + h
            state = (jnp.zeros((HD, HD), F32), jnp.zeros((1, HD), F32), jnp.full((1, LANES), NEG, F32))
            total = jnp.zeros((1, LANES), F32)
            for j in order(d):
                state = advance(state, i, j)
                total = total + abuf[j, 2 * heads + i:2 * heads + i + 1]
            stsend[d, h * HD:(h + 1) * HD] = state[0].astype(BF16)
            stsend[d, heads * HD + 16 * h:heads * HD + 16 * h + 16] = jnp.broadcast_to(state[1], (16, HD)).astype(BF16)
            scsend[d, h:h + 1] = state[2]
            scsend[d, heads + h:heads + h + 1] = total

    def state_copies(d, to):
        return (
            pltpu.make_async_remote_copy(
                src_ref=stsend.at[d], dst_ref=strecv.at[e], send_sem=s_send.at[to], recv_sem=s_recv.at[e],
                device_id=(to, t), device_id_type=MESH),
            pltpu.make_async_remote_copy(
                src_ref=scsend.at[d], dst_ref=screcv.at[e], send_sem=c_send.at[to], recv_sem=c_recv.at[e],
                device_id=(to, t), device_id_type=MESH),
        )

    def start_states(d):
        def one(to, carry):
            for c in state_copies(d, to):
                c.start()
            return carry
        return one

    lax.fori_loop(e + 1, E, start_states(0), 0)
    lax.fori_loop(0, e, start_states(1), 0)

    def forward(k):
        s = lax.rem(e - k + E, E)
        return pltpu.make_async_remote_copy(
            src_ref=xin.at[lo, s], dst_ref=xin.at[lo, s], send_sem=f_send.at[k], recv_sem=f_recv.at[k],
            device_id=(e, mate), device_id_type=MESH)

    own.wait()
    forward(0).start()

    def pass_on(k, carry):
        dispatch(k).wait_recv()
        forward(k).start()
        return carry

    lax.fori_loop(1, E, pass_on, 0)
    for i in range(5, 8):
        loads[H + i].wait()

    def give_half(k):
        s = lax.rem(e - k + E, E)
        return pltpu.make_async_remote_copy(
            src_ref=yboth.at[s, 1 - lo], dst_ref=yrecv.at[s], send_sem=y_send.at[k], recv_sem=y_recv.at[k],
            device_id=(e, mate), device_id_type=MESH)

    def give_back(k):
        s = lax.rem(e - k + E, E)
        return pltpu.make_async_remote_copy(
            src_ref=retsend.at[s], dst_ref=ret.at[e], send_sem=r_send.at[k], recv_sem=r_recv.at[k],
            device_id=(s, t), device_id_type=MESH)

    def finish(k):
        s = lax.rem(e - k + E, E)
        give_half(k).wait_recv()
        retsend[s] = (yboth[s, lo].astype(F32) + yrecv[s].astype(F32)).astype(BF16)
        give_back(k).start()

    def expert(k):
        s = lax.rem(e - k + E, E)
        forward(k).wait_recv()
        rows = xin[:, s].reshape(2 * R, D)
        gate = nn(rows, wgv[...])
        up = nn(rows, wuv[...])
        hid = (gate * jax.nn.sigmoid(gate) * up).astype(BF16)
        for c in range(0, D, CHUNK):
            y = nn(hid, wdv[:, c:c + CHUNK]).astype(BF16)
            yboth[s, :, :, c:c + CHUNK] = y.reshape(2, R, CHUNK)
        give_half(k).start()

    expert(1)

    def steps(k, carry):
        expert(k)
        finish(k - 1)
        return carry

    lax.fori_loop(2, E, steps, 0)
    expert(0)
    finish(E - 1)
    give_half(0).wait_recv()
    ret[e] = (yboth[e, lo].astype(F32) + yrecv[e].astype(F32)).astype(BF16)

    def wait_states(j, carry):
        pltpu.make_async_copy(strecv.at[j], strecv.at[j], s_recv.at[j]).wait()
        pltpu.make_async_copy(screcv.at[j], screcv.at[j], c_recv.at[j]).wait()
        return carry

    lax.fori_loop(0, e, wait_states, 0)
    lax.fori_loop(e + 1, E, wait_states, 0)

    def join(j, carry):
        out = []
        for h in range(heads):
            mem, nor, m = carry[3 * h:3 * h + 3]
            m_j = screcv[j, h:h + 1]
            base = m + screcv[j, heads + h:heads + h + 1]
            g = jnp.maximum(base, m_j)
            old, new = jnp.exp(base - g), jnp.exp(m_j - g)
            c_j = strecv[j, h * HD:(h + 1) * HD].astype(F32)
            n_j = strecv[j, heads * HD + 16 * h:heads * HD + 16 * h + 16].astype(F32)[0:1]
            out += [old * mem + new * c_j, old * nor + new * n_j, g]
        return tuple(out)

    zero = (jnp.zeros((HD, HD), F32), jnp.zeros((1, HD), F32), jnp.zeros((1, LANES), F32)) * heads
    for d in range(2):
        if d == 0:
            entry = lax.fori_loop(0, e, join, zero)
        else:
            entry = lax.fori_loop(0, E - 1 - e, lambda i, c: join(E - 1 - i, c), zero)
        for h in range(heads):
            i = d * heads + h
            state = entry[3 * h:3 * h + 3]
            for n, j in enumerate(order(d)):
                cin[j, i] = state[0].astype(BF16)
                nin[j, i:i + 1] = state[1]
                min_[j, i:i + 1] = state[2]
                if n < NB - 1:
                    state = advance(state, i, j)

    def mix(j, carry):
        at = pl.ds(pl.multiple_of(j * BLK, BLK), BLK)
        rows = rowsv[j]
        cols = colsv[j]
        for h in range(heads):
            hs = slice(h * HD, (h + 1) * HD)
            q, k, v = qs[at, hs], ks[at, hs], vs[at, hs]
            raw = nt(q, k)
            q_wide = q.astype(F32)
            both = None
            for d in range(2):
                i = d * heads + h
                mask = (pos_r >= pos_c) if d == 0 else (pos_r <= pos_c)
                a = jnp.where(mask, rows[i:i + 1], NEG)
                m_in = min_[j, i:i + 1][:, 0:1]
                g = jnp.maximum(jnp.max(a, axis=1, keepdims=True), m_in)
                s = raw * jnp.exp(a - g)
                w = jnp.exp(m_in - g)
                num = nn(s.astype(BF16), v) + w * nn(q, cin[j, i])
                den = jnp.sum(s, axis=1, keepdims=True) + w * jnp.sum(q_wide * nin[j, i:i + 1], axis=1, keepdims=True)
                floor = jnp.exp(-(cols[:, 2 * heads + i:2 * heads + i + 1] + g))
                part = num / jnp.maximum(jnp.abs(den), floor)
                both = part if both is None else both + part
            gated = jax.nn.sigmoid(os_[at, hs].astype(F32)) * both
            hsend[at, hs] = rms(gated, head_gain[:, hs]).astype(BF16)
        return carry

    lax.fori_loop(0, NB, mix, 0)
    MR = hsend.shape[0] // TP

    def share_h(k):
        to = lax.rem(t + k, TP)
        return pltpu.make_async_remote_copy(
            src_ref=hsend.at[pl.ds(pl.multiple_of(to * MR, MR), MR)], dst_ref=hrecv.at[t],
            send_sem=h_send.at[k], recv_sem=h_recv.at[k], device_id=(e, to), device_id_type=MESH)

    for k in range(1, TP):
        share_h(k).start()
    hrecv[t] = hsend[pl.ds(pl.multiple_of(t * MR, MR), MR), :]
    for k in range(1, TP):
        share_w(k).wait_recv()
        share_h(k).wait_recv()
    for c in range(0, D, CHUNK):
        acc = nn(hrecv[0], wfull[0, :, c:c + CHUNK])
        for g in range(1, TP):
            acc = acc + nn(hrecv[g], wfull[g, :, c:c + CHUNK])
        mixer_out[:, c:c + CHUNK] = acc.astype(BF16)

    for k in range(1, H):
        share_g(k).wait_recv()
    for k in range(1, E):
        give_back(k).wait_recv()

    def chosen(h):
        place = lax.broadcasted_iota(jnp.int32, (quarter, slots), 1)
        mat = None
        for j in range(TOPK):
            term = jnp.where(place == slot_v[h, j][:, 0:1], wts[h][:, j:j + 1], 0.0)
            mat = term if mat is None else mat + term
        return mat.astype(BF16)

    mats = [chosen(h) for h in range(H)]
    for h in range(H):
        for c in range(0, D, CHUNK):
            got = ret[:, h * cap:(h + 1) * cap, c:c + CHUNK].reshape(slots, CHUNK)
            outsend[h, :, c:c + CHUNK] = nn(mats[h], got).astype(BF16)

    def share_o(k):
        to = lax.rem(hi + k, H)
        return pltpu.make_async_remote_copy(
            src_ref=outsend.at[to], dst_ref=outrecv.at[hi], send_sem=o_send.at[k], recv_sem=o_recv.at[k],
            device_id=(e, 2 * to + lo), device_id_type=MESH)

    for k in range(1, H):
        share_o(k).start()
    total = outsend[hi].astype(F32)
    for k in range(1, H):
        share_o(k).wait_recv()
        total = total + outrecv[lax.rem(hi - k + H, H)].astype(F32)
    route_out[...] = total.astype(BF16)

    for k in range(1, E):
        dispatch(k).wait_send()
        give_back(k).wait_send()
    for k in range(E):
        forward(k).wait_send()
        give_half(k).wait_send()
    for k in range(1, TP):
        share_w(k).wait_send()
        share_h(k).wait_send()
    for k in range(1, H):
        share_g(k).wait_send()
        share_o(k).wait_send()

    def end_states(d):
        def one(to, carry):
            for c in state_copies(d, to):
                c.wait_send()
            return carry
        return one

    lax.fori_loop(e + 1, E, end_states(0), 0)
    lax.fori_loop(0, e, end_states(1), 0)


def shards(
    x_mix, mix_gain, w_query, w_key, w_value, w_outgate, w_gates, gate_bias, gate_drift,
    head_gain, w_out, x_route, route_gain, routes, route_weight, w_gate_e, w_up_e, w_down_e,
):
    E = lax.axis_size("ep")
    TP = lax.axis_size("tp")
    t = lax.axis_index("tp")
    rows, D = x_mix.shape
    width = w_query.shape[1]
    heads = width // HD
    NB = rows // BLK
    quarter = x_route.shape[0] // TP
    cap = 2 * quarter * TOPK // E
    H = TP // 2
    R = H * cap
    FH = w_gate_e.shape[2]
    MR = rows // TP
    own = lax.dynamic_slice_in_dim(w_gates.reshape(D, 4, -1), t * heads, heads, 2)
    gates_t = own.reshape(D, 4 * heads).T
    kind = jnp.arange(4, dtype=jnp.int32) % 2
    add = gate_bias[None] + gate_drift[:, None, None] * kind[None, :, None].astype(F32)
    add = jnp.broadcast_to(add.reshape(NB, 4 * heads, 1), (NB, 4 * heads, BLK))
    weights = jnp.pad(route_weight, ((0, 0), (0, LANES - TOPK)))
    anywhere = pl.BlockSpec(memory_space=pl.ANY)
    vmem = pl.BlockSpec(memory_space=pltpu.VMEM)
    V = pltpu.VMEM
    dma = pltpu.SemaphoreType.DMA
    SR = heads * HD + 16 * heads
    scratch = [
        V((rows, D), BF16), V((D, width), BF16), V((D, width), BF16), V((D, width), BF16), V((D, width), BF16),
        V((H, quarter, D), BF16), V((D, FH), BF16), V((D, FH), BF16), V((FH, D), BF16),
        V((TP, width, D), BF16), V((H, quarter, LANES), F32),
        V((E, R, D), BF16), V((2, E, R, D), BF16), V((E, 2, R, D), BF16), V((E, R, D), BF16),
        V((E, R, D), BF16), V((E, R, D), BF16), V((H, quarter, D), BF16), V((H, quarter, D), BF16),
        V((rows, width), BF16), V((rows, width), BF16), V((rows, width), BF16), V((rows, width), BF16),
        V((NB, 4 * heads, BLK), F32), V((NB, BLK, 4 * heads), F32), V((NB, 4 * heads, LANES), F32),
        V((NB, 2 * heads, HD, HD), F32), V((NB, 2 * heads, HD), F32),
        V((2, SR, HD), BF16), V((2, 8, LANES), F32), V((E, SR, HD), BF16), V((E, 8, LANES), F32),
        V((NB, 2 * heads, HD, HD), BF16), V((NB, 2 * heads, HD), F32), V((NB, 2 * heads, LANES), F32),
        V((rows, width), BF16), V((TP, MR, width), BF16), V((H, TOPK, quarter, LANES), jnp.int32),
        dma((H + 10,)), dma((1,)),
    ] + [dma((E,))] * 12 + [dma((TP,))] * 4 + [dma((H,))] * 4
    return pl.pallas_call(
        functools.partial(body, E, TP, heads, cap, quarter),
        out_shape=(jax.ShapeDtypeStruct((MR, D), BF16), jax.ShapeDtypeStruct((quarter, D), BF16)),
        in_specs=[anywhere] * 10 + [vmem] * 6 + [anywhere],
        out_specs=(vmem, vmem),
        scratch_shapes=scratch,
        compiler_params=pltpu.CompilerParams(
            collective_id=0, has_side_effects=True, vmem_limit_bytes=67043328),
    )(
        x_mix, w_query, w_key, w_value, w_outgate, x_route, w_gate_e[0], w_up_e[0], w_down_e[0], w_out,
        mix_gain[None], route_gain[None], head_gain[None], gates_t, add, routes, weights,
    )


def solution(mesh):
    return jax.shard_map(
        shards,
        mesh=mesh,
        in_specs=(
            P("ep", None), P(), P(None, "tp"), P(None, "tp"), P(None, "tp"), P(None, "tp"), P(),
            P(None, "tp"), P("ep"), P("tp"), P("tp", None), P("ep", None), P(), P("ep", None),
            P(("ep", "tp"), None), P("ep", None, "tp"), P("ep", None, "tp"), P("ep", "tp", None),
        ),
        out_specs=(P(("ep", "tp"), None), P(("ep", "tp"), None)),
        check_vma=False,
    )
```

```python
import functools

import jax
import jax.numpy as jnp
from jax import lax
from jax.experimental import pallas as pl
from jax.experimental.pallas import tpu as pltpu
from jax.sharding import PartitionSpec as P

HD = 128
TOPK = 2
BLK = 256
EPS = 1e-06
NEG = -1e30
MESH = pl.DeviceIdType.MESH
F32 = jnp.float32
BF16 = jnp.bfloat16
LANES = 128
CHUNK = 512


def nn(a, b):
    return lax.dot_general(a, b, (((1,), (0,)), ((), ())), preferred_element_type=F32)


def nt(a, b):
    return lax.dot_general(a, b, (((1,), (1,)), ((), ())), preferred_element_type=F32)


def tn(a, b):
    return lax.dot_general(a, b, (((0,), (0,)), ((), ())), preferred_element_type=F32)


def rms(rows, gain):
    rows = rows.astype(F32)
    return rows * lax.rsqrt(jnp.mean(rows * rows, axis=-1, keepdims=True) + EPS) * gain


def body(
    E, TP, heads, cap, quarter,
    x_mix, wq, wk, wv, wo, x_route, wg_e, wu_e, wd_e, w_out,
    mix_gain, route_gain, head_gain, w_gates, gate_add, routes, weights,
    mixer_out, route_out,
    xm, wqv, wkv, wvv, wov, xr, wgv, wuv, wdv, wfull,
    sendbuf, xin, hid, retsend, ret,
    qs, ks, vs, os_, rowsv, colsv, abuf, kvb, nb, stsend, scsend, strecv, screcv,
    cin, nin, min_, hsend, hrecv, slot_v,
    lsem, own_sem, d_send, d_recv, r_send, r_recv,
    s_send, s_recv, c_send, c_recv, h_send, h_recv, wx_send, wx_recv, wm_send, wm_recv,
):
    e = lax.axis_index("ep")
    t = lax.axis_index("tp")
    lo = lax.rem(t, 2)
    mate = t + 1 - 2 * lo
    H = TP // 2
    D = xm.shape[1]
    NB = xm.shape[0] // BLK
    slots = E * cap
    parts = ((wg_e, wgv), (wu_e, wuv), (wd_e, wdv), (w_out, wfull))

    loads = []
    for i, (src, dst) in enumerate([
        (x_route.at[pl.ds(t * quarter, quarter)], xr), (x_mix, xm), (wq, wqv), (wk, wkv), (wv, wvv), (wo, wov),
    ] + [(src, dst.at[t]) for src, dst in parts]):
        loads.append(pltpu.make_async_copy(src, dst, lsem.at[i]))
    for c in loads:
        c.start()

    barrier = pltpu.get_barrier_semaphore()
    for k in range(1, E):
        pl.semaphore_signal(barrier, inc=1, device_id=(lax.rem(e + k, E), t), device_id_type=MESH)
    for k in range(1, TP):
        pl.semaphore_signal(barrier, inc=1, device_id=(e, lax.rem(t + k, TP)), device_id_type=MESH)
    pl.semaphore_wait(barrier, E - 1 + TP - 1)

    def across(i, k):
        src, dst = parts[i]
        return pltpu.make_async_remote_copy(
            src_ref=src, dst_ref=dst.at[t], send_sem=wx_send.at[i, k], recv_sem=wx_recv.at[i, k],
            device_id=(e, lax.rem(t + 2 * k, TP)), device_id_type=MESH)

    def to_mate(i, k):
        src, dst = parts[i]
        whose = lax.rem(t - 2 * k + TP, TP)
        return pltpu.make_async_remote_copy(
            src_ref=src if k == 0 else dst.at[whose], dst_ref=dst.at[whose],
            send_sem=wm_send.at[i, k], recv_sem=wm_recv.at[i, k], device_id=(e, mate), device_id_type=MESH)

    for i in range(4):
        for k in range(1, H):
            across(i, k).start()

    tri = (lax.broadcasted_iota(jnp.int32, (quarter, quarter), 0)
           > lax.broadcasted_iota(jnp.int32, (quarter, quarter), 1)).astype(BF16)
    loads[0].wait()
    table = routes[pl.ds(t * quarter, quarter), :]
    experts = lax.broadcasted_iota(jnp.int32, (quarter, E), 1)
    hot = [(experts == table[:, j:j + 1]).astype(F32) for j in range(TOPK)]
    before = nn(tri, sum(hot).astype(BF16))
    place = lax.broadcasted_iota(jnp.int32, (quarter, slots), 1)
    pick = None
    for j in range(TOPK):
        slot = table[:, j:j + 1] * cap + jnp.sum(before * hot[j], axis=1, keepdims=True).astype(jnp.int32)
        slot_v[j] = jnp.broadcast_to(slot, (quarter, LANES))
        here = (place == slot).astype(F32)
        pick = here if pick is None else pick + here
    pick = pick.astype(BF16)
    normed_rows = rms(xr[...], route_gain[...]).astype(BF16)
    for c in range(0, D, CHUNK):
        packed = tn(pick, normed_rows[:, c:c + CHUNK]).astype(BF16)
        sendbuf[:, :, c:c + CHUNK] = packed.reshape(E, cap, CHUNK)

    def dispatch(k):
        to = lax.rem(e + k, E)
        return pltpu.make_async_remote_copy(
            src_ref=sendbuf.at[to], dst_ref=xin.at[e], send_sem=d_send.at[k], recv_sem=d_recv.at[k],
            device_id=(to, t), device_id_type=MESH)

    own = pltpu.make_async_copy(sendbuf.at[e], xin.at[e], own_sem.at[0])
    own.start()
    for k in range(1, E):
        dispatch(k).start()
    for i in range(4):
        to_mate(i, 0).start()

    for i in range(1, 6):
        loads[i].wait()
    pos_r = lax.broadcasted_iota(jnp.int32, (BLK, BLK), 0)
    pos_c = lax.broadcasted_iota(jnp.int32, (BLK, BLK), 1)

    def project(j, carry):
        at = pl.ds(pl.multiple_of(j * BLK, BLK), BLK)
        normed = rms(xm[at, :], mix_gain[...]).astype(BF16)
        qs[at, :] = nn(normed, wqv[...]).astype(BF16)
        k_all = (nn(normed, wkv[...]) * (HD ** -0.5)).astype(BF16)
        v_all = nn(normed, wvv[...]).astype(BF16)
        ks[at, :] = k_all
        vs[at, :] = v_all
        os_[at, :] = nn(normed, wov[...]).astype(BF16)
        pre = nt(w_gates[...], normed) + gate_add[j]
        logf = jnp.minimum(pre, 0.0) - jnp.log1p(jnp.exp(-jnp.abs(pre)))
        upper = (pos_r <= pos_c).astype(F32)
        lower = (pos_r >= pos_c).astype(F32)
        cum = jnp.dot(logf, upper, precision=lax.Precision.HIGHEST, preferred_element_type=F32)
        rev = jnp.dot(logf, lower, precision=lax.Precision.HIGHEST, preferred_element_type=F32)
        b_fw = cum[heads:2 * heads]
        b_bw = rev[3 * heads:4 * heads]
        a_fw = pre[0:heads] - b_fw
        a_bw = pre[2 * heads:3 * heads] - b_bw
        rows = jnp.concatenate([a_fw, a_bw, b_fw, b_bw], axis=0)
        cols = jnp.transpose(rows)
        rowsv[j] = rows
        colsv[j] = cols
        scal = []
        for d in range(2):
            for h in range(heads):
                i = d * heads + h
                top = jnp.max(rows[i:i + 1], axis=1, keepdims=True)
                scal.append(jnp.broadcast_to(top, (1, LANES)))
                w_col = jnp.exp(cols[:, i:i + 1] - top)
                hs = slice(h * HD, (h + 1) * HD)
                kw = k_all[:, hs].astype(F32) * w_col
                kvb[j, i] = tn(kw.astype(BF16), v_all[:, hs])
                nb[j, i:i + 1] = jnp.sum(kw, axis=0, keepdims=True)
        for d in range(2):
            for h in range(heads):
                i = 2 * heads + d * heads + h
                end = rows[i:i + 1, BLK - 1:BLK] if d == 0 else rows[i:i + 1, 0:1]
                scal.append(jnp.broadcast_to(end, (1, LANES)))
        abuf[j] = jnp.concatenate(scal, axis=0)
        return carry

    lax.fori_loop(0, NB, project, 0)

    def advance(state, i, j):
        mem, nor, m = state
        top = abuf[j, i:i + 1]
        tot = abuf[j, 2 * heads + i:2 * heads + i + 1]
        g = jnp.maximum(m, top)
        old, new = jnp.exp(m - g), jnp.exp(top - g)
        return (old * mem + new * kvb[j, i], old * nor + new * nb[j, i:i + 1], tot + g)

    def order(d):
        return range(NB) if d == 0 else range(NB - 1, -1, -1)

    for d in range(2):
        for h in range(heads):
            i = d * heads + h
            state = (jnp.zeros((HD, HD), F32), jnp.zeros((1, HD), F32), jnp.full((1, LANES), NEG, F32))
            total = jnp.zeros((1, LANES), F32)
            for j in order(d):
                state = advance(state, i, j)
                total = total + abuf[j, 2 * heads + i:2 * heads + i + 1]
            stsend[d, h * HD:(h + 1) * HD] = state[0].astype(BF16)
            stsend[d, heads * HD + 16 * h:heads * HD + 16 * h + 16] = jnp.broadcast_to(state[1], (16, HD)).astype(BF16)
            scsend[d, h:h + 1] = state[2]
            scsend[d, heads + h:heads + h + 1] = total

    def state_copies(d, to):
        return (
            pltpu.make_async_remote_copy(
                src_ref=stsend.at[d], dst_ref=strecv.at[e], send_sem=s_send.at[to], recv_sem=s_recv.at[e],
                device_id=(to, t), device_id_type=MESH),
            pltpu.make_async_remote_copy(
                src_ref=scsend.at[d], dst_ref=screcv.at[e], send_sem=c_send.at[to], recv_sem=c_recv.at[e],
                device_id=(to, t), device_id_type=MESH),
        )

    def start_states(d):
        def one(to, carry):
            for c in state_copies(d, to):
                c.start()
            return carry
        return one

    lax.fori_loop(e + 1, E, start_states(0), 0)
    lax.fori_loop(0, e, start_states(1), 0)

    own.wait()
    for k in range(1, E):
        dispatch(k).wait_recv()

    def hidden(g):
        rows = xin[...].reshape(slots, D)
        gate = nn(rows, wgv[g])
        up = nn(rows, wuv[g])
        hid[g] = (gate * jax.nn.sigmoid(gate) * up).astype(BF16)

    for i in range(6, 10):
        loads[i].wait()
    hidden(t)
    for i in range(2):
        to_mate(i, 0).wait_recv()
    hidden(mate)
    for k in range(1, H):
        for i in range(2):
            across(i, k).wait_recv()
            to_mate(i, k).start()
        hidden(lax.rem(t - 2 * k + TP, TP))
        for i in range(2):
            to_mate(i, k).wait_recv()
        hidden(lax.rem(mate - 2 * k + TP, TP))

    def wait_states(j, carry):
        pltpu.make_async_copy(strecv.at[j], strecv.at[j], s_recv.at[j]).wait()
        pltpu.make_async_copy(screcv.at[j], screcv.at[j], c_recv.at[j]).wait()
        return carry

    lax.fori_loop(0, e, wait_states, 0)
    lax.fori_loop(e + 1, E, wait_states, 0)

    def join(j, carry):
        out = []
        for h in range(heads):
            mem, nor, m = carry[3 * h:3 * h + 3]
            m_j = screcv[j, h:h + 1]
            base = m + screcv[j, heads + h:heads + h + 1]
            g = jnp.maximum(base, m_j)
            old, new = jnp.exp(base - g), jnp.exp(m_j - g)
            c_j = strecv[j, h * HD:(h + 1) * HD].astype(F32)
            n_j = strecv[j, heads * HD + 16 * h:heads * HD + 16 * h + 16].astype(F32)[0:1]
            out += [old * mem + new * c_j, old * nor + new * n_j, g]
        return tuple(out)

    zero = (jnp.zeros((HD, HD), F32), jnp.zeros((1, HD), F32), jnp.zeros((1, LANES), F32)) * heads
    for d in range(2):
        if d == 0:
            entry = lax.fori_loop(0, e, join, zero)
        else:
            entry = lax.fori_loop(0, E - 1 - e, lambda i, c: join(E - 1 - i, c), zero)
        for h in range(heads):
            i = d * heads + h
            state = entry[3 * h:3 * h + 3]
            for n, j in enumerate(order(d)):
                cin[j, i] = state[0].astype(BF16)
                nin[j, i:i + 1] = state[1]
                min_[j, i:i + 1] = state[2]
                if n < NB - 1:
                    state = advance(state, i, j)

    def mix(j, carry):
        at = pl.ds(pl.multiple_of(j * BLK, BLK), BLK)
        rows = rowsv[j]
        cols = colsv[j]
        for h in range(heads):
            hs = slice(h * HD, (h + 1) * HD)
            q, k, v = qs[at, hs], ks[at, hs], vs[at, hs]
            raw = nt(q, k)
            q_wide = q.astype(F32)
            both = None
            for d in range(2):
                i = d * heads + h
                mask = (pos_r >= pos_c) if d == 0 else (pos_r <= pos_c)
                a = jnp.where(mask, rows[i:i + 1], NEG)
                m_in = min_[j, i:i + 1][:, 0:1]
                g = jnp.maximum(jnp.max(a, axis=1, keepdims=True), m_in)
                s = raw * jnp.exp(a - g)
                w = jnp.exp(m_in - g)
                num = nn(s.astype(BF16), v) + w * nn(q, cin[j, i])
                den = jnp.sum(s, axis=1, keepdims=True) + w * jnp.sum(q_wide * nin[j, i:i + 1], axis=1, keepdims=True)
                floor = jnp.exp(-(cols[:, 2 * heads + i:2 * heads + i + 1] + g))
                part = num / jnp.maximum(jnp.abs(den), floor)
                both = part if both is None else both + part
            gated = jax.nn.sigmoid(os_[at, hs].astype(F32)) * both
            hsend[at, hs] = rms(gated, head_gain[:, hs]).astype(BF16)
        return carry

    lax.fori_loop(0, NB, mix, 0)
    MR = hsend.shape[0] // TP

    def share_h(k):
        to = lax.rem(t + k, TP)
        return pltpu.make_async_remote_copy(
            src_ref=hsend.at[pl.ds(pl.multiple_of(to * MR, MR), MR)], dst_ref=hrecv.at[t],
            send_sem=h_send.at[k], recv_sem=h_recv.at[k], device_id=(e, to), device_id_type=MESH)

    for k in range(1, TP):
        share_h(k).start()
    hrecv[t] = hsend[pl.ds(pl.multiple_of(t * MR, MR), MR), :]

    for k in range(1, H):
        across(2, k).wait_recv()
        to_mate(2, k).start()
    for k in range(H):
        to_mate(2, k).wait_recv()

    def give_back(k):
        s = lax.rem(e + k, E)
        return pltpu.make_async_remote_copy(
            src_ref=retsend.at[s], dst_ref=ret.at[e], send_sem=r_send.at[k], recv_sem=r_recv.at[k],
            device_id=(s, t), device_id_type=MESH)

    group = max(1, 2 * LANES // cap)
    span = group * cap
    for n in range(E // group):
        first = lax.rem(e // group + n + 1, E // group)
        at = pl.ds(pl.multiple_of(first * span, span), span)
        for c in range(0, D, CHUNK):
            y = nn(hid[0, at, :], wdv[0, :, c:c + CHUNK])
            for g in range(1, TP):
                y = y + nn(hid[g, at, :], wdv[g, :, c:c + CHUNK])
            retsend[pl.ds(first * group, group), :, c:c + CHUNK] = y.astype(BF16).reshape(group, cap, CHUNK)
        for m in range(group):
            s = first * group + m

            @pl.when(s != e)
            def _():
                give_back(lax.rem(s - e + E, E)).start()

    ret[e] = retsend[e]

    for k in range(1, H):
        across(3, k).wait_recv()
        to_mate(3, k).start()
    for k in range(H):
        to_mate(3, k).wait_recv()
    for k in range(1, TP):
        share_h(k).wait_recv()
    for c in range(0, D, CHUNK):
        acc = nn(hrecv[0], wfull[0, :, c:c + CHUNK])
        for g in range(1, TP):
            acc = acc + nn(hrecv[g], wfull[g, :, c:c + CHUNK])
        mixer_out[:, c:c + CHUNK] = acc.astype(BF16)

    for k in range(1, E):
        give_back(k).wait_recv()
    mat = None
    for j in range(TOPK):
        term = jnp.where(place == slot_v[j][:, 0:1], weights[:, j:j + 1], 0.0)
        mat = term if mat is None else mat + term
    mat = mat.astype(BF16)
    for c in range(0, D, CHUNK):
        got = ret[:, :, c:c + CHUNK].reshape(slots, CHUNK)
        route_out[:, c:c + CHUNK] = nn(mat, got).astype(BF16)

    for k in range(1, E):
        dispatch(k).wait_send()
        give_back(k).wait_send()
    for i in range(4):
        for k in range(1, H):
            across(i, k).wait_send()
        for k in range(H):
            to_mate(i, k).wait_send()
    for k in range(1, TP):
        share_h(k).wait_send()

    def end_states(d):
        def one(to, carry):
            for c in state_copies(d, to):
                c.wait_send()
            return carry
        return one

    lax.fori_loop(e + 1, E, end_states(0), 0)
    lax.fori_loop(0, e, end_states(1), 0)


def shards(
    x_mix, mix_gain, w_query, w_key, w_value, w_outgate, w_gates, gate_bias, gate_drift,
    head_gain, w_out, x_route, route_gain, routes, route_weight, w_gate_e, w_up_e, w_down_e,
):
    E = lax.axis_size("ep")
    TP = lax.axis_size("tp")
    t = lax.axis_index("tp")
    rows, D = x_mix.shape
    width = w_query.shape[1]
    heads = width // HD
    NB = rows // BLK
    quarter = x_route.shape[0] // TP
    cap = 2 * quarter * TOPK // E
    H = TP // 2
    FH = w_gate_e.shape[2]
    MR = rows // TP
    own = lax.dynamic_slice_in_dim(w_gates.reshape(D, 4, -1), t * heads, heads, 2)
    gates_t = own.reshape(D, 4 * heads).T
    kind = jnp.arange(4, dtype=jnp.int32) % 2
    add = gate_bias[None] + gate_drift[:, None, None] * kind[None, :, None].astype(F32)
    add = jnp.broadcast_to(add.reshape(NB, 4 * heads, 1), (NB, 4 * heads, BLK))
    anywhere = pl.BlockSpec(memory_space=pl.ANY)
    vmem = pl.BlockSpec(memory_space=pltpu.VMEM)
    V = pltpu.VMEM
    dma = pltpu.SemaphoreType.DMA
    SR = heads * HD + 16 * heads
    scratch = [
        V((rows, D), BF16), V((D, width), BF16), V((D, width), BF16), V((D, width), BF16), V((D, width), BF16),
        V((quarter, D), BF16), V((TP, D, FH), BF16), V((TP, D, FH), BF16), V((TP, FH, D), BF16),
        V((TP, width, D), BF16),
        V((E, cap, D), BF16), V((E, cap, D), BF16), V((TP, E * cap, FH), BF16), V((E, cap, D), BF16),
        V((E, cap, D), BF16),
        V((rows, width), BF16), V((rows, width), BF16), V((rows, width), BF16), V((rows, width), BF16),
        V((NB, 4 * heads, BLK), F32), V((NB, BLK, 4 * heads), F32), V((NB, 4 * heads, LANES), F32),
        V((NB, 2 * heads, HD, HD), F32), V((NB, 2 * heads, HD), F32),
        V((2, SR, HD), BF16), V((2, 8, LANES), F32), V((E, SR, HD), BF16), V((E, 8, LANES), F32),
        V((NB, 2 * heads, HD, HD), BF16), V((NB, 2 * heads, HD), F32), V((NB, 2 * heads, LANES), F32),
        V((rows, width), BF16), V((TP, MR, width), BF16), V((TOPK, quarter, LANES), jnp.int32),
        dma((10,)), dma((1,)),
    ] + [dma((E,))] * 8 + [dma((TP,))] * 2 + [dma((4, H))] * 4
    return pl.pallas_call(
        functools.partial(body, E, TP, heads, cap, quarter),
        out_shape=(jax.ShapeDtypeStruct((MR, D), BF16), jax.ShapeDtypeStruct((quarter, D), BF16)),
        in_specs=[anywhere] * 10 + [vmem] * 7,
        out_specs=(vmem, vmem),
        scratch_shapes=scratch,
        compiler_params=pltpu.CompilerParams(
            collective_id=0, has_side_effects=True, vmem_limit_bytes=67043328),
    )(
        x_mix, w_query, w_key, w_value, w_outgate, x_route, w_gate_e[0], w_up_e[0], w_down_e[0], w_out,
        mix_gain[None], route_gain[None], head_gain[None], gates_t, add, routes, route_weight,
    )


def solution(mesh):
    return jax.shard_map(
        shards,
        mesh=mesh,
        in_specs=(
            P("ep", None), P(), P(None, "tp"), P(None, "tp"), P(None, "tp"), P(None, "tp"), P(),
            P(None, "tp"), P("ep"), P("tp"), P("tp", None), P("ep", None), P(), P("ep", None),
            P(("ep", "tp"), None), P("ep", None, "tp"), P("ep", None, "tp"), P("ep", "tp", None),
        ),
        out_specs=(P(("ep", "tp"), None), P(("ep", "tp"), None)),
        check_vma=False,
    )
```

```python
import functools

import jax
import jax.numpy as jnp
from jax import lax
from jax.experimental import pallas as pl
from jax.experimental.pallas import tpu as pltpu
from jax.sharding import PartitionSpec as P

HD = 128
TOPK = 2
BLK = 256
EPS = 1e-06
NEG = -1e30
MESH = pl.DeviceIdType.MESH
F32 = jnp.float32
BF16 = jnp.bfloat16
LANES = 128
CHUNK = 512


def nn(a, b):
    return lax.dot_general(a, b, (((1,), (0,)), ((), ())), preferred_element_type=F32)


def nt(a, b):
    return lax.dot_general(a, b, (((1,), (1,)), ((), ())), preferred_element_type=F32)


def tn(a, b):
    return lax.dot_general(a, b, (((0,), (0,)), ((), ())), preferred_element_type=F32)


def rms(rows, gain):
    rows = rows.astype(F32)
    return rows * lax.rsqrt(jnp.mean(rows * rows, axis=-1, keepdims=True) + EPS) * gain


def body(
    E, TP, heads, cap, quarter,
    x_mix, wq, wk, wv, wo, x_route, wg_e, wu_e, wd_e, w_out,
    mix_gain, route_gain, head_gain, w_gates, gate_bias, gate_drift, routes, weights,
    mixer_out, route_out,
    xm, wqv, wkv, wvv, wov, xr, wgv, wuv, wdv, wfull,
    sendbuf, xin, hid, retsend, ret,
    qs, ks, vs, os_, rowsv, colsv, abuf, kvb, nb, stsend, scsend, strecv, screcv,
    cin, nin, min_, hsend, hrecv, slot_v, gate_add, gate_w,
    lsem, own_sem, d_send, d_recv, r_send, r_recv,
    s_send, s_recv, c_send, c_recv, h_send, h_recv, wx_send, wx_recv, wm_send, wm_recv,
):
    e = lax.axis_index("ep")
    t = lax.axis_index("tp")
    lo = lax.rem(t, 2)
    mate = t + 1 - 2 * lo
    H = TP // 2
    D = xm.shape[1]
    NB = xm.shape[0] // BLK
    slots = E * cap
    half = wd_e.shape[0] // 2
    parts = (
        (wg_e, wgv), (wu_e, wuv),
        (wd_e.at[pl.ds(0, half)], wdv.at[:, pl.ds(0, half)]),
        (wd_e.at[pl.ds(half, half)], wdv.at[:, pl.ds(half, half)]),
        (w_out, wfull),
    )
    n_parts = len(parts)

    loads = []
    for i, (src, dst) in enumerate([
        (x_route.at[pl.ds(t * quarter, quarter)], xr), (x_mix, xm), (wq, wqv), (wk, wkv), (wv, wvv), (wo, wov),
    ] + [(src, dst.at[t]) for src, dst in parts]):
        loads.append(pltpu.make_async_copy(src, dst, lsem.at[i]))
    for c in loads:
        c.start()

    barrier = pltpu.get_barrier_semaphore()
    for k in range(1, E):
        pl.semaphore_signal(barrier, inc=1, device_id=(lax.rem(e + k, E), t), device_id_type=MESH)
    for k in range(1, TP):
        pl.semaphore_signal(barrier, inc=1, device_id=(e, lax.rem(t + k, TP)), device_id_type=MESH)
    pl.semaphore_wait(barrier, E - 1 + TP - 1)

    def across(i, k):
        src, dst = parts[i]
        return pltpu.make_async_remote_copy(
            src_ref=src, dst_ref=dst.at[t], send_sem=wx_send.at[i, k], recv_sem=wx_recv.at[i, k],
            device_id=(e, lax.rem(t + 2 * k, TP)), device_id_type=MESH)

    def to_mate(i, k):
        src, dst = parts[i]
        whose = lax.rem(t - 2 * k + TP, TP)
        return pltpu.make_async_remote_copy(
            src_ref=src if k == 0 else dst.at[whose], dst_ref=dst.at[whose],
            send_sem=wm_send.at[i, k], recv_sem=wm_recv.at[i, k], device_id=(e, mate), device_id_type=MESH)

    for i in range(n_parts):
        for k in range(1, H):
            across(i, k).start()

    tri = (lax.broadcasted_iota(jnp.int32, (quarter, quarter), 0)
           < lax.broadcasted_iota(jnp.int32, (quarter, quarter), 1)).astype(BF16)
    loads[0].wait()
    place = lax.broadcasted_iota(jnp.int32, (slots, quarter), 0)
    experts = lax.broadcasted_iota(jnp.int32, (E, quarter), 0)
    table = routes[:, pl.ds(pl.multiple_of(t * quarter, quarter), quarter)]
    hot = [(experts == table[j:j + 1]).astype(F32) for j in range(TOPK)]
    before = nn(sum(hot).astype(BF16), tri)
    pick = None
    for j in range(TOPK):
        slot = table[j:j + 1] * cap + jnp.sum(before * hot[j], axis=0, keepdims=True).astype(jnp.int32)
        slot_v[j:j + 1] = slot
        here = (place == slot).astype(F32)
        pick = here if pick is None else pick + here
    pick = pick.astype(BF16)
    normed_rows = rms(xr[...], route_gain[...]).astype(BF16)
    for c in range(0, D, CHUNK):
        packed = nn(pick, normed_rows[:, c:c + CHUNK]).astype(BF16)
        sendbuf[:, :, c:c + CHUNK] = packed.reshape(E, cap, CHUNK)

    def dispatch(k):
        to = lax.rem(e + k, E)
        return pltpu.make_async_remote_copy(
            src_ref=sendbuf.at[to], dst_ref=xin.at[e], send_sem=d_send.at[k], recv_sem=d_recv.at[k],
            device_id=(to, t), device_id_type=MESH)

    own = pltpu.make_async_copy(sendbuf.at[e], xin.at[e], own_sem.at[0])
    own.start()
    for k in range(1, E):
        dispatch(k).start()
    for i in range(n_parts):
        to_mate(i, 0).start()

    for i in range(1, 6):
        loads[i].wait()
    pos_r = lax.broadcasted_iota(jnp.int32, (BLK, BLK), 0)
    pos_c = lax.broadcasted_iota(jnp.int32, (BLK, BLK), 1)

    width = w_gates.shape[0] // 4
    row = lax.broadcasted_iota(jnp.int32, (4 * heads, 4 * width), 0)
    col = lax.broadcasted_iota(jnp.int32, (4 * heads, 4 * width), 1)
    own_rows = None
    for g in range(4):
        for h in range(heads):
            here = ((row == g * heads + h) & (col == g * width + t * heads + h)).astype(F32)
            own_rows = here if own_rows is None else own_rows + here
    gate_w[...] = nn(own_rows.astype(BF16), w_gates[...]).astype(BF16)
    for j in range(NB):
        for g in range(4):
            for h in range(heads):
                value = gate_bias[h:h + 1, g:g + 1]
                if g % 2 == 1:
                    value = value + gate_drift[:, j:j + 1]
                gate_add[j, g * heads + h:g * heads + h + 1] = jnp.broadcast_to(value, (1, BLK))

    def project(j, carry):
        at = pl.ds(pl.multiple_of(j * BLK, BLK), BLK)
        normed = rms(xm[at, :], mix_gain[...]).astype(BF16)
        qs[at, :] = nn(normed, wqv[...]).astype(BF16)
        k_all = (nn(normed, wkv[...]) * (HD ** -0.5)).astype(BF16)
        v_all = nn(normed, wvv[...]).astype(BF16)
        ks[at, :] = k_all
        vs[at, :] = v_all
        os_[at, :] = nn(normed, wov[...]).astype(BF16)
        pre = nt(gate_w[...], normed) + gate_add[j]
        logf = jnp.minimum(pre, 0.0) - jnp.log1p(jnp.exp(-jnp.abs(pre)))
        upper = (pos_r <= pos_c).astype(F32)
        lower = (pos_r >= pos_c).astype(F32)
        cum = jnp.dot(logf, upper, precision=lax.Precision.HIGHEST, preferred_element_type=F32)
        rev = jnp.dot(logf, lower, precision=lax.Precision.HIGHEST, preferred_element_type=F32)
        b_fw = cum[heads:2 * heads]
        b_bw = rev[3 * heads:4 * heads]
        a_fw = pre[0:heads] - b_fw
        a_bw = pre[2 * heads:3 * heads] - b_bw
        rows = jnp.concatenate([a_fw, a_bw, b_fw, b_bw], axis=0)
        cols = jnp.transpose(rows)
        rowsv[j] = rows
        colsv[j] = cols
        scal = []
        for d in range(2):
            for h in range(heads):
                i = d * heads + h
                top = jnp.max(rows[i:i + 1], axis=1, keepdims=True)
                scal.append(jnp.broadcast_to(top, (1, LANES)))
                w_col = jnp.exp(cols[:, i:i + 1] - top)
                hs = slice(h * HD, (h + 1) * HD)
                kw = k_all[:, hs].astype(F32) * w_col
                kvb[j, i] = tn(kw.astype(BF16), v_all[:, hs])
                nb[j, i:i + 1] = jnp.sum(kw, axis=0, keepdims=True)
        for d in range(2):
            for h in range(heads):
                i = 2 * heads + d * heads + h
                end = rows[i:i + 1, BLK - 1:BLK] if d == 0 else rows[i:i + 1, 0:1]
                scal.append(jnp.broadcast_to(end, (1, LANES)))
        abuf[j] = jnp.concatenate(scal, axis=0)
        return carry

    lax.fori_loop(0, NB, project, 0)

    def advance(state, i, j):
        mem, nor, m = state
        top = abuf[j, i:i + 1]
        tot = abuf[j, 2 * heads + i:2 * heads + i + 1]
        g = jnp.maximum(m, top)
        old, new = jnp.exp(m - g), jnp.exp(top - g)
        return (old * mem + new * kvb[j, i], old * nor + new * nb[j, i:i + 1], tot + g)

    def order(d):
        return range(NB) if d == 0 else range(NB - 1, -1, -1)

    for d in range(2):
        for h in range(heads):
            i = d * heads + h
            state = (jnp.zeros((HD, HD), F32), jnp.zeros((1, HD), F32), jnp.full((1, LANES), NEG, F32))
            total = jnp.zeros((1, LANES), F32)
            for j in order(d):
                state = advance(state, i, j)
                total = total + abuf[j, 2 * heads + i:2 * heads + i + 1]
            stsend[d, h * HD:(h + 1) * HD] = state[0].astype(BF16)
            stsend[d, heads * HD + 16 * h:heads * HD + 16 * h + 16] = jnp.broadcast_to(state[1], (16, HD)).astype(BF16)
            scsend[d, h:h + 1] = state[2]
            scsend[d, heads + h:heads + h + 1] = total

    def state_copies(d, to):
        return (
            pltpu.make_async_remote_copy(
                src_ref=stsend.at[d], dst_ref=strecv.at[e], send_sem=s_send.at[to], recv_sem=s_recv.at[e],
                device_id=(to, t), device_id_type=MESH),
            pltpu.make_async_remote_copy(
                src_ref=scsend.at[d], dst_ref=screcv.at[e], send_sem=c_send.at[to], recv_sem=c_recv.at[e],
                device_id=(to, t), device_id_type=MESH),
        )

    def start_states(d):
        def one(to, carry):
            for c in state_copies(d, to):
                c.start()
            return carry
        return one

    lax.fori_loop(e + 1, E, start_states(0), 0)
    lax.fori_loop(0, e, start_states(1), 0)

    own.wait()
    for k in range(1, E):
        dispatch(k).wait_recv()

    def hidden(g):
        rows = xin[...].reshape(slots, D)
        gate = nn(rows, wgv[g])
        up = nn(rows, wuv[g])
        hid[g] = (gate * jax.nn.sigmoid(gate) * up).astype(BF16)

    for i in range(6, 6 + n_parts):
        loads[i].wait()
    hidden(t)
    for i in range(2):
        to_mate(i, 0).wait_recv()
    hidden(mate)
    for k in range(1, H):
        for i in range(2):
            across(i, k).wait_recv()
            to_mate(i, k).start()
        hidden(lax.rem(t - 2 * k + TP, TP))
        for i in range(2):
            to_mate(i, k).wait_recv()
        hidden(lax.rem(mate - 2 * k + TP, TP))

    for i in (2, 3):
        for k in range(1, H):
            across(i, k).wait_recv()
            to_mate(i, k).start()
    for i in (2, 3):
        for k in range(H):
            to_mate(i, k).wait_recv()

    def give_back(k):
        s = lax.rem(e + k, E)
        return pltpu.make_async_remote_copy(
            src_ref=retsend.at[s], dst_ref=ret.at[e], send_sem=r_send.at[k], recv_sem=r_recv.at[k],
            device_id=(s, t), device_id_type=MESH)

    group = max(1, 2 * LANES // cap)
    span = group * cap
    for n in range(E // group):
        first = lax.rem(e // group + n + 1, E // group)
        at = pl.ds(pl.multiple_of(first * span, span), span)
        for c in range(0, D, CHUNK):
            y = nn(hid[0, at, :], wdv[0, :, c:c + CHUNK])
            for g in range(1, TP):
                y = y + nn(hid[g, at, :], wdv[g, :, c:c + CHUNK])
            retsend[pl.ds(first * group, group), :, c:c + CHUNK] = y.astype(BF16).reshape(group, cap, CHUNK)
        for m in range(group):
            s = first * group + m

            @pl.when(s != e)
            def _():
                give_back(lax.rem(s - e + E, E)).start()

    ret[e] = retsend[e]

    def wait_states(j, carry):
        pltpu.make_async_copy(strecv.at[j], strecv.at[j], s_recv.at[j]).wait()
        pltpu.make_async_copy(screcv.at[j], screcv.at[j], c_recv.at[j]).wait()
        return carry

    lax.fori_loop(0, e, wait_states, 0)
    lax.fori_loop(e + 1, E, wait_states, 0)

    def join(j, carry):
        out = []
        for h in range(heads):
            mem, nor, m = carry[3 * h:3 * h + 3]
            m_j = screcv[j, h:h + 1]
            base = m + screcv[j, heads + h:heads + h + 1]
            g = jnp.maximum(base, m_j)
            old, new = jnp.exp(base - g), jnp.exp(m_j - g)
            c_j = strecv[j, h * HD:(h + 1) * HD].astype(F32)
            n_j = strecv[j, heads * HD + 16 * h:heads * HD + 16 * h + 16].astype(F32)[0:1]
            out += [old * mem + new * c_j, old * nor + new * n_j, g]
        return tuple(out)

    zero = (jnp.zeros((HD, HD), F32), jnp.zeros((1, HD), F32), jnp.zeros((1, LANES), F32)) * heads
    for d in range(2):
        if d == 0:
            entry = lax.fori_loop(0, e, join, zero)
        else:
            entry = lax.fori_loop(0, E - 1 - e, lambda i, c: join(E - 1 - i, c), zero)
        for h in range(heads):
            i = d * heads + h
            state = entry[3 * h:3 * h + 3]
            for n, j in enumerate(order(d)):
                cin[j, i] = state[0].astype(BF16)
                nin[j, i:i + 1] = state[1]
                min_[j, i:i + 1] = state[2]
                if n < NB - 1:
                    state = advance(state, i, j)

    def mix(j, carry):
        at = pl.ds(pl.multiple_of(j * BLK, BLK), BLK)
        rows = rowsv[j]
        cols = colsv[j]
        for h in range(heads):
            hs = slice(h * HD, (h + 1) * HD)
            q, k, v = qs[at, hs], ks[at, hs], vs[at, hs]
            raw = nt(q, k)
            q_wide = q.astype(F32)
            both = None
            for d in range(2):
                i = d * heads + h
                mask = (pos_r >= pos_c) if d == 0 else (pos_r <= pos_c)
                a = jnp.where(mask, rows[i:i + 1], NEG)
                m_in = min_[j, i:i + 1][:, 0:1]
                g = jnp.maximum(jnp.max(a, axis=1, keepdims=True), m_in)
                s = raw * jnp.exp(a - g)
                w = jnp.exp(m_in - g)
                num = nn(s.astype(BF16), v) + w * nn(q, cin[j, i])
                den = jnp.sum(s, axis=1, keepdims=True) + w * jnp.sum(q_wide * nin[j, i:i + 1], axis=1, keepdims=True)
                floor = jnp.exp(-(cols[:, 2 * heads + i:2 * heads + i + 1] + g))
                part = num / jnp.maximum(jnp.abs(den), floor)
                both = part if both is None else both + part
            gated = jax.nn.sigmoid(os_[at, hs].astype(F32)) * both
            hsend[at, hs] = rms(gated, head_gain[:, hs]).astype(BF16)
        return carry

    lax.fori_loop(0, NB, mix, 0)
    MR = hsend.shape[0] // TP

    def share_h(k):
        to = lax.rem(t + k, TP)
        return pltpu.make_async_remote_copy(
            src_ref=hsend.at[pl.ds(pl.multiple_of(to * MR, MR), MR)], dst_ref=hrecv.at[t],
            send_sem=h_send.at[k], recv_sem=h_recv.at[k], device_id=(e, to), device_id_type=MESH)

    for k in range(1, TP):
        share_h(k).start()
    hrecv[t] = hsend[pl.ds(pl.multiple_of(t * MR, MR), MR), :]

    for k in range(1, H):
        across(4, k).wait_recv()
        to_mate(4, k).start()
    for k in range(H):
        to_mate(4, k).wait_recv()
    for k in range(1, TP):
        share_h(k).wait_recv()
    for c in range(0, D, CHUNK):
        acc = nn(hrecv[0], wfull[0, :, c:c + CHUNK])
        for g in range(1, TP):
            acc = acc + nn(hrecv[g], wfull[g, :, c:c + CHUNK])
        mixer_out[:, c:c + CHUNK] = acc.astype(BF16)

    for k in range(1, E):
        give_back(k).wait_recv()
    mat = None
    for j in range(TOPK):
        term = jnp.where(place == slot_v[j:j + 1], weights[j:j + 1], 0.0)
        mat = term if mat is None else mat + term
    mat = mat.astype(BF16)
    for c in range(0, D, CHUNK):
        got = ret[:, :, c:c + CHUNK].reshape(slots, CHUNK)
        route_out[:, c:c + CHUNK] = tn(mat, got).astype(BF16)

    for k in range(1, E):
        dispatch(k).wait_send()
        give_back(k).wait_send()
    for i in range(n_parts):
        for k in range(1, H):
            across(i, k).wait_send()
        for k in range(H):
            to_mate(i, k).wait_send()
    for k in range(1, TP):
        share_h(k).wait_send()

    def end_states(d):
        def one(to, carry):
            for c in state_copies(d, to):
                c.wait_send()
            return carry
        return one

    lax.fori_loop(e + 1, E, end_states(0), 0)
    lax.fori_loop(0, e, end_states(1), 0)


def shards(
    x_mix, mix_gain, w_query, w_key, w_value, w_outgate, w_gates, gate_bias, gate_drift,
    head_gain, w_out, x_route, route_gain, routes, route_weight, w_gate_e, w_up_e, w_down_e,
):
    E = lax.axis_size("ep")
    TP = lax.axis_size("tp")
    rows, D = x_mix.shape
    width = w_query.shape[1]
    heads = width // HD
    NB = rows // BLK
    quarter = x_route.shape[0] // TP
    cap = 2 * quarter * TOPK // E
    H = TP // 2
    FH = w_gate_e.shape[2]
    MR = rows // TP
    anywhere = pl.BlockSpec(memory_space=pl.ANY)
    vmem = pl.BlockSpec(memory_space=pltpu.VMEM)
    V = pltpu.VMEM
    dma = pltpu.SemaphoreType.DMA
    SR = heads * HD + 16 * heads
    scratch = [
        V((rows, D), BF16), V((D, width), BF16), V((D, width), BF16), V((D, width), BF16), V((D, width), BF16),
        V((quarter, D), BF16), V((TP, D, FH), BF16), V((TP, D, FH), BF16), V((TP, FH, D), BF16),
        V((TP, width, D), BF16),
        V((E, cap, D), BF16), V((E, cap, D), BF16), V((TP, E * cap, FH), BF16), V((E, cap, D), BF16),
        V((E, cap, D), BF16),
        V((rows, width), BF16), V((rows, width), BF16), V((rows, width), BF16), V((rows, width), BF16),
        V((NB, 4 * heads, BLK), F32), V((NB, BLK, 4 * heads), F32), V((NB, 4 * heads, LANES), F32),
        V((NB, 2 * heads, HD, HD), F32), V((NB, 2 * heads, HD), F32),
        V((2, SR, HD), BF16), V((2, 8, LANES), F32), V((E, SR, HD), BF16), V((E, 8, LANES), F32),
        V((NB, 2 * heads, HD, HD), BF16), V((NB, 2 * heads, HD), F32), V((NB, 2 * heads, LANES), F32),
        V((rows, width), BF16), V((TP, MR, width), BF16), V((TOPK, quarter), jnp.int32), V((NB, 4 * heads, BLK), F32), V((4 * heads, D), BF16),
        dma((11,)), dma((1,)),
    ] + [dma((E,))] * 8 + [dma((TP,))] * 2 + [dma((5, H))] * 4
    return pl.pallas_call(
        functools.partial(body, E, TP, heads, cap, quarter),
        out_shape=(jax.ShapeDtypeStruct((MR, D), BF16), jax.ShapeDtypeStruct((quarter, D), BF16)),
        in_specs=[anywhere] * 10 + [vmem] * 8,
        out_specs=(vmem, vmem),
        scratch_shapes=scratch,
        compiler_params=pltpu.CompilerParams(
            collective_id=0, has_side_effects=True, vmem_limit_bytes=67043328),
    )(
        x_mix, w_query, w_key, w_value, w_outgate, x_route, w_gate_e[0], w_up_e[0], w_down_e[0], w_out,
        mix_gain[None], route_gain[None], head_gain[None], w_gates.T, gate_bias.T, gate_drift[None], routes.T,
        route_weight.T,
    )


def solution(mesh):
    return jax.shard_map(
        shards,
        mesh=mesh,
        in_specs=(
            P("ep", None), P(), P(None, "tp"), P(None, "tp"), P(None, "tp"), P(None, "tp"), P(),
            P(None, "tp"), P("ep"), P("tp"), P("tp", None), P("ep", None), P(), P("ep", None),
            P(("ep", "tp"), None), P("ep", None, "tp"), P("ep", None, "tp"), P("ep", "tp", None),
        ),
        out_specs=(P(("ep", "tp"), None), P(("ep", "tp"), None)),
        check_vma=False,
    )
```

```python
import functools

import jax
import jax.numpy as jnp
from jax import lax
from jax.experimental import pallas as pl
from jax.experimental.pallas import tpu as pltpu
from jax.sharding import PartitionSpec as P

HD = 128
TOPK = 2
BLK = 256
EPS = 1e-06
NEG = -1e30
MESH = pl.DeviceIdType.MESH
F32 = jnp.float32
BF16 = jnp.bfloat16
LANES = 128
CHUNK = 512


def nn(a, b):
    return lax.dot_general(a, b, (((1,), (0,)), ((), ())), preferred_element_type=F32)


def nt(a, b):
    return lax.dot_general(a, b, (((1,), (1,)), ((), ())), preferred_element_type=F32)


def tn(a, b):
    return lax.dot_general(a, b, (((0,), (0,)), ((), ())), preferred_element_type=F32)


def rms(rows, gain):
    rows = rows.astype(F32)
    return rows * lax.rsqrt(jnp.mean(rows * rows, axis=-1, keepdims=True) + EPS) * gain


def body(
    E, TP, heads, cap, quarter,
    x_mix, wq, wk, wv, wo, x_route, wg_e, wu_e, wd_e, w_out,
    mix_gain, route_gain, head_gain, w_gates, gate_bias, gate_drift, routes, weights,
    mixer_out, route_out,
    xm, wqv, wkv, wvv, wov, xr, wgv, wuv, wdv, wfull,
    sendbuf, xin, hid, fsend, frecv, nsend, nrecv, psend, precv, meta_s, meta_r,
    qs, ks, vs, os_, rowsv, colsv, abuf, kvb, nb, stsend, scsend, strecv, screcv,
    cin, nin, min_, hsend, hrecv, slot_v, gate_add, gate_w,
    lsem, own_sem, d_send, d_recv,
    s_send, s_recv, c_send, c_recv, h_send, h_recv, wx_send, wx_recv, wm_send, wm_recv,
    f_send, f_recv, n_send, n_recv, p_send, p_recv, m_send, m_recv,
):
    e = lax.axis_index("ep")
    t = lax.axis_index("tp")
    lo = lax.rem(t, 2)
    mate = t + 1 - 2 * lo
    H = TP // 2
    D = xm.shape[1]
    NB = xm.shape[0] // BLK
    slots = E * cap
    E2 = E // 2
    span = E2 * cap
    side = lax.div(e, E2)
    me = lax.rem(e, E2)
    base = side * E2
    pal = lax.rem(e + E2, E)
    half = wd_e.shape[0] // 2
    parts = (
        (wg_e, wgv), (wu_e, wuv),
        (wd_e.at[pl.ds(0, half)], wdv.at[:, pl.ds(0, half)]),
        (wd_e.at[pl.ds(half, half)], wdv.at[:, pl.ds(half, half)]),
        (w_out, wfull),
    )
    n_parts = len(parts)

    loads = []
    for i, (src, dst) in enumerate([
        (x_route.at[pl.ds(t * quarter, quarter)], xr), (x_mix, xm), (wq, wqv), (wk, wkv), (wv, wvv), (wo, wov),
    ] + [(src, dst.at[t]) for src, dst in parts]):
        loads.append(pltpu.make_async_copy(src, dst, lsem.at[i]))
    for c in loads:
        c.start()

    barrier = pltpu.get_barrier_semaphore()
    for k in range(1, E):
        pl.semaphore_signal(barrier, inc=1, device_id=(lax.rem(e + k, E), t), device_id_type=MESH)
    for k in range(1, TP):
        pl.semaphore_signal(barrier, inc=1, device_id=(e, lax.rem(t + k, TP)), device_id_type=MESH)
    pl.semaphore_wait(barrier, E - 1 + TP - 1)

    def across(i, k):
        src, dst = parts[i]
        return pltpu.make_async_remote_copy(
            src_ref=src, dst_ref=dst.at[t], send_sem=wx_send.at[i, k], recv_sem=wx_recv.at[i, k],
            device_id=(e, lax.rem(t + 2 * k, TP)), device_id_type=MESH)

    def to_mate(i, k):
        src, dst = parts[i]
        whose = lax.rem(t - 2 * k + TP, TP)
        return pltpu.make_async_remote_copy(
            src_ref=src if k == 0 else dst.at[whose], dst_ref=dst.at[whose],
            send_sem=wm_send.at[i, k], recv_sem=wm_recv.at[i, k], device_id=(e, mate), device_id_type=MESH)

    for i in range(n_parts):
        for k in range(1, H):
            across(i, k).start()

    tri = (lax.broadcasted_iota(jnp.int32, (quarter, quarter), 0)
           < lax.broadcasted_iota(jnp.int32, (quarter, quarter), 1)).astype(BF16)
    loads[0].wait()
    place = lax.broadcasted_iota(jnp.int32, (slots, quarter), 0)
    experts = lax.broadcasted_iota(jnp.int32, (E, quarter), 0)
    table = routes[:, pl.ds(pl.multiple_of(t * quarter, quarter), quarter)]
    hot = [(experts == table[j:j + 1]).astype(F32) for j in range(TOPK)]
    before = nn(sum(hot).astype(BF16), tri)
    pick = None
    for j in range(TOPK):
        slot = table[j:j + 1] * cap + jnp.sum(before * hot[j], axis=0, keepdims=True).astype(jnp.int32)
        slot_v[j:j + 1] = slot - base * cap
        meta_s[j:j + 1] = (slot - (1 - side) * span).astype(F32)
        meta_s[TOPK + j:TOPK + j + 1] = weights[j:j + 1]
        here = (place == slot).astype(F32)
        pick = here if pick is None else pick + here
    pick = pick.astype(BF16)
    normed_rows = rms(xr[...], route_gain[...]).astype(BF16)
    for c in range(0, D, CHUNK):
        packed = nn(pick, normed_rows[:, c:c + CHUNK]).astype(BF16)
        sendbuf[:, :, c:c + CHUNK] = packed.reshape(E, cap, CHUNK)

    def dispatch(k):
        to = lax.rem(e + k, E)
        return pltpu.make_async_remote_copy(
            src_ref=sendbuf.at[to], dst_ref=xin.at[e], send_sem=d_send.at[k], recv_sem=d_recv.at[k],
            device_id=(to, t), device_id_type=MESH)

    own = pltpu.make_async_copy(sendbuf.at[e], xin.at[e], own_sem.at[0])
    own.start()
    meta = pltpu.make_async_remote_copy(
        src_ref=meta_s, dst_ref=meta_r, send_sem=m_send.at[0], recv_sem=m_recv.at[0],
        device_id=(pal, t), device_id_type=MESH)
    meta.start()
    for k in range(1, E):
        dispatch(k).start()
    for i in range(n_parts):
        to_mate(i, 0).start()

    for i in range(1, 6):
        loads[i].wait()
    pos_r = lax.broadcasted_iota(jnp.int32, (BLK, BLK), 0)
    pos_c = lax.broadcasted_iota(jnp.int32, (BLK, BLK), 1)

    width = w_gates.shape[0] // 4
    row = lax.broadcasted_iota(jnp.int32, (4 * heads, 4 * width), 0)
    col = lax.broadcasted_iota(jnp.int32, (4 * heads, 4 * width), 1)
    own_rows = None
    for g in range(4):
        for h in range(heads):
            here = ((row == g * heads + h) & (col == g * width + t * heads + h)).astype(F32)
            own_rows = here if own_rows is None else own_rows + here
    gate_w[...] = nn(own_rows.astype(BF16), w_gates[...]).astype(BF16)
    for j in range(NB):
        for g in range(4):
            for h in range(heads):
                value = gate_bias[h:h + 1, g:g + 1]
                if g % 2 == 1:
                    value = value + gate_drift[:, j:j + 1]
                gate_add[j, g * heads + h:g * heads + h + 1] = jnp.broadcast_to(value, (1, BLK))

    def project(j, carry):
        at = pl.ds(pl.multiple_of(j * BLK, BLK), BLK)
        normed = rms(xm[at, :], mix_gain[...]).astype(BF16)
        qs[at, :] = nn(normed, wqv[...]).astype(BF16)
        k_all = (nn(normed, wkv[...]) * (HD ** -0.5)).astype(BF16)
        v_all = nn(normed, wvv[...]).astype(BF16)
        ks[at, :] = k_all
        vs[at, :] = v_all
        os_[at, :] = nn(normed, wov[...]).astype(BF16)
        pre = nt(gate_w[...], normed) + gate_add[j]
        logf = jnp.minimum(pre, 0.0) - jnp.log1p(jnp.exp(-jnp.abs(pre)))
        upper = (pos_r <= pos_c).astype(F32)
        lower = (pos_r >= pos_c).astype(F32)
        cum = jnp.dot(logf, upper, precision=lax.Precision.HIGHEST, preferred_element_type=F32)
        rev = jnp.dot(logf, lower, precision=lax.Precision.HIGHEST, preferred_element_type=F32)
        b_fw = cum[heads:2 * heads]
        b_bw = rev[3 * heads:4 * heads]
        a_fw = pre[0:heads] - b_fw
        a_bw = pre[2 * heads:3 * heads] - b_bw
        rows = jnp.concatenate([a_fw, a_bw, b_fw, b_bw], axis=0)
        cols = jnp.transpose(rows)
        rowsv[j] = rows
        colsv[j] = cols
        scal = []
        for d in range(2):
            for h in range(heads):
                i = d * heads + h
                top = jnp.max(rows[i:i + 1], axis=1, keepdims=True)
                scal.append(jnp.broadcast_to(top, (1, LANES)))
                w_col = jnp.exp(cols[:, i:i + 1] - top)
                hs = slice(h * HD, (h + 1) * HD)
                kw = k_all[:, hs].astype(F32) * w_col
                kvb[j, i] = tn(kw.astype(BF16), v_all[:, hs])
                nb[j, i:i + 1] = jnp.sum(kw, axis=0, keepdims=True)
        for d in range(2):
            for h in range(heads):
                i = 2 * heads + d * heads + h
                end = rows[i:i + 1, BLK - 1:BLK] if d == 0 else rows[i:i + 1, 0:1]
                scal.append(jnp.broadcast_to(end, (1, LANES)))
        abuf[j] = jnp.concatenate(scal, axis=0)
        return carry

    lax.fori_loop(0, NB, project, 0)

    def advance(state, i, j):
        mem, nor, m = state
        top = abuf[j, i:i + 1]
        tot = abuf[j, 2 * heads + i:2 * heads + i + 1]
        g = jnp.maximum(m, top)
        old, new = jnp.exp(m - g), jnp.exp(top - g)
        return (old * mem + new * kvb[j, i], old * nor + new * nb[j, i:i + 1], tot + g)

    def order(d):
        return range(NB) if d == 0 else range(NB - 1, -1, -1)

    for d in range(2):
        for h in range(heads):
            i = d * heads + h
            state = (jnp.zeros((HD, HD), F32), jnp.zeros((1, HD), F32), jnp.full((1, LANES), NEG, F32))
            total = jnp.zeros((1, LANES), F32)
            for j in order(d):
                state = advance(state, i, j)
                total = total + abuf[j, 2 * heads + i:2 * heads + i + 1]
            stsend[d, h * HD:(h + 1) * HD] = state[0].astype(BF16)
            stsend[d, heads * HD + 16 * h:heads * HD + 16 * h + 16] = jnp.broadcast_to(state[1], (16, HD)).astype(BF16)
            scsend[d, h:h + 1] = state[2]
            scsend[d, heads + h:heads + h + 1] = total

    def state_copies(d, to):
        return (
            pltpu.make_async_remote_copy(
                src_ref=stsend.at[d], dst_ref=strecv.at[e], send_sem=s_send.at[to], recv_sem=s_recv.at[e],
                device_id=(to, t), device_id_type=MESH),
            pltpu.make_async_remote_copy(
                src_ref=scsend.at[d], dst_ref=screcv.at[e], send_sem=c_send.at[to], recv_sem=c_recv.at[e],
                device_id=(to, t), device_id_type=MESH),
        )

    def start_states(d):
        def one(to, carry):
            for c in state_copies(d, to):
                c.start()
            return carry
        return one

    lax.fori_loop(e + 1, E, start_states(0), 0)
    lax.fori_loop(0, e, start_states(1), 0)

    own.wait()
    for k in range(1, E):
        dispatch(k).wait_recv()

    def hidden(g):
        rows = xin[...].reshape(slots, D)
        gate = nn(rows, wgv[g])
        up = nn(rows, wuv[g])
        hid[g] = (gate * jax.nn.sigmoid(gate) * up).astype(BF16)

    for i in range(6, 6 + n_parts):
        loads[i].wait()
    hidden(t)
    for i in range(2):
        to_mate(i, 0).wait_recv()
    hidden(mate)
    for k in range(1, H):
        for i in range(2):
            across(i, k).wait_recv()
            to_mate(i, k).start()
        hidden(lax.rem(t - 2 * k + TP, TP))
        for i in range(2):
            to_mate(i, k).wait_recv()
        hidden(lax.rem(mate - 2 * k + TP, TP))

    def wait_states(j, carry):
        pltpu.make_async_copy(strecv.at[j], strecv.at[j], s_recv.at[j]).wait()
        pltpu.make_async_copy(screcv.at[j], screcv.at[j], c_recv.at[j]).wait()
        return carry

    lax.fori_loop(0, e, wait_states, 0)
    lax.fori_loop(e + 1, E, wait_states, 0)

    def join(j, carry):
        out = []
        for h in range(heads):
            mem, nor, m = carry[3 * h:3 * h + 3]
            m_j = screcv[j, h:h + 1]
            base = m + screcv[j, heads + h:heads + h + 1]
            g = jnp.maximum(base, m_j)
            old, new = jnp.exp(base - g), jnp.exp(m_j - g)
            c_j = strecv[j, h * HD:(h + 1) * HD].astype(F32)
            n_j = strecv[j, heads * HD + 16 * h:heads * HD + 16 * h + 16].astype(F32)[0:1]
            out += [old * mem + new * c_j, old * nor + new * n_j, g]
        return tuple(out)

    zero = (jnp.zeros((HD, HD), F32), jnp.zeros((1, HD), F32), jnp.zeros((1, LANES), F32)) * heads
    for d in range(2):
        if d == 0:
            entry = lax.fori_loop(0, e, join, zero)
        else:
            entry = lax.fori_loop(0, E - 1 - e, lambda i, c: join(E - 1 - i, c), zero)
        for h in range(heads):
            i = d * heads + h
            state = entry[3 * h:3 * h + 3]
            for n, j in enumerate(order(d)):
                cin[j, i] = state[0].astype(BF16)
                nin[j, i:i + 1] = state[1]
                min_[j, i:i + 1] = state[2]
                if n < NB - 1:
                    state = advance(state, i, j)

    def mix(j, carry):
        at = pl.ds(pl.multiple_of(j * BLK, BLK), BLK)
        rows = rowsv[j]
        cols = colsv[j]
        for h in range(heads):
            hs = slice(h * HD, (h + 1) * HD)
            q, k, v = qs[at, hs], ks[at, hs], vs[at, hs]
            raw = nt(q, k)
            q_wide = q.astype(F32)
            both = None
            for d in range(2):
                i = d * heads + h
                mask = (pos_r >= pos_c) if d == 0 else (pos_r <= pos_c)
                a = jnp.where(mask, rows[i:i + 1], NEG)
                m_in = min_[j, i:i + 1][:, 0:1]
                g = jnp.maximum(jnp.max(a, axis=1, keepdims=True), m_in)
                s = raw * jnp.exp(a - g)
                w = jnp.exp(m_in - g)
                num = nn(s.astype(BF16), v) + w * nn(q, cin[j, i])
                den = jnp.sum(s, axis=1, keepdims=True) + w * jnp.sum(q_wide * nin[j, i:i + 1], axis=1, keepdims=True)
                floor = jnp.exp(-(cols[:, 2 * heads + i:2 * heads + i + 1] + g))
                part = num / jnp.maximum(jnp.abs(den), floor)
                both = part if both is None else both + part
            gated = jax.nn.sigmoid(os_[at, hs].astype(F32)) * both
            hsend[at, hs] = rms(gated, head_gain[:, hs]).astype(BF16)
        return carry

    lax.fori_loop(0, NB, mix, 0)
    MR = hsend.shape[0] // TP

    def share_h(k):
        to = lax.rem(t + k, TP)
        return pltpu.make_async_remote_copy(
            src_ref=hsend.at[pl.ds(pl.multiple_of(to * MR, MR), MR)], dst_ref=hrecv.at[t],
            send_sem=h_send.at[k], recv_sem=h_recv.at[k], device_id=(e, to), device_id_type=MESH)

    for k in range(1, TP):
        share_h(k).start()
    hrecv[t] = hsend[pl.ds(pl.multiple_of(t * MR, MR), MR), :]

    for i in (2, 3):
        for k in range(1, H):
            across(i, k).wait_recv()
            to_mate(i, k).start()
    for i in (2, 3):
        for k in range(H):
            to_mate(i, k).wait_recv()

    def far(c, k):
        m = lax.rem(me + k, E2)
        return pltpu.make_async_remote_copy(
            src_ref=fsend.at[c, m], dst_ref=frecv.at[c, me], send_sem=f_send.at[c, k], recv_sem=f_recv.at[c, k],
            device_id=(base + m, t), device_id_type=MESH)

    def near(k):
        m = lax.rem(me + k, E2)
        return pltpu.make_async_remote_copy(
            src_ref=nsend.at[m], dst_ref=nrecv.at[me], send_sem=n_send.at[k], recv_sem=n_recv.at[k],
            device_id=(base + m, t), device_id_type=MESH)

    def part_sum(c):
        return pltpu.make_async_remote_copy(
            src_ref=psend.at[c], dst_ref=precv.at[c], send_sem=p_send.at[c], recv_sem=p_recv.at[c],
            device_id=(pal, t), device_id_type=MESH)

    def results(first, c):
        at = pl.ds(pl.multiple_of(first * cap, span), span)
        cols = slice(c * CHUNK, (c + 1) * CHUNK)
        y = nn(hid[0, at, :], wdv[0, :, cols])
        for g in range(1, TP):
            y = y + nn(hid[g, at, :], wdv[g, :, cols])
        return y.astype(BF16).reshape(E2, cap, CHUNK)

    NCH = D // CHUNK
    for c in range(NCH):
        fsend[c] = results((1 - side) * E2, c)
        for k in range(1, E2):
            far(c, k).start()
        frecv[c, me] = fsend[c, me]
    for c in range(NCH):
        nsend[:, :, c * CHUNK:(c + 1) * CHUNK] = results(base, c)
    for k in range(1, E2):
        near(k).start()
    nrecv[me] = nsend[me]

    def weigh(slot_rows, weight_rows):
        at = lax.broadcasted_iota(jnp.int32, (span, quarter), 0).astype(slot_rows[0].dtype)
        mat = None
        for j in range(TOPK):
            term = jnp.where(at == slot_rows[j], weight_rows[j], 0.0)
            mat = term if mat is None else mat + term
        return mat.astype(BF16)

    meta.wait_recv()
    theirs = weigh([meta_r[j:j + 1] for j in range(TOPK)], [meta_r[TOPK + j:TOPK + j + 1] for j in range(TOPK)])
    for c in range(NCH):
        for k in range(1, E2):
            far(c, k).wait_recv()
        psend[c] = tn(theirs, frecv[c].reshape(span, CHUNK)).astype(BF16)
        part_sum(c).start()

    for k in range(1, H):
        across(4, k).wait_recv()
        to_mate(4, k).start()
    for k in range(H):
        to_mate(4, k).wait_recv()
    for k in range(1, TP):
        share_h(k).wait_recv()
    for c in range(0, D, CHUNK):
        acc = nn(hrecv[0], wfull[0, :, c:c + CHUNK])
        for g in range(1, TP):
            acc = acc + nn(hrecv[g], wfull[g, :, c:c + CHUNK])
        mixer_out[:, c:c + CHUNK] = acc.astype(BF16)

    for k in range(1, E2):
        near(k).wait_recv()
    ours = weigh([slot_v[j:j + 1] for j in range(TOPK)], [weights[j:j + 1] for j in range(TOPK)])
    for c in range(NCH):
        cols = slice(c * CHUNK, (c + 1) * CHUNK)
        kept = tn(ours, nrecv[:, :, cols].reshape(span, CHUNK))
        part_sum(c).wait_recv()
        route_out[:, cols] = (kept + precv[c].astype(F32)).astype(BF16)

    for k in range(1, E):
        dispatch(k).wait_send()
    for i in range(n_parts):
        for k in range(1, H):
            across(i, k).wait_send()
        for k in range(H):
            to_mate(i, k).wait_send()
    for k in range(1, TP):
        share_h(k).wait_send()
    meta.wait_send()
    for k in range(1, E2):
        near(k).wait_send()
    for c in range(NCH):
        part_sum(c).wait_send()
        for k in range(1, E2):
            far(c, k).wait_send()

    def end_states(d):
        def one(to, carry):
            for c in state_copies(d, to):
                c.wait_send()
            return carry
        return one

    lax.fori_loop(e + 1, E, end_states(0), 0)
    lax.fori_loop(0, e, end_states(1), 0)


def shards(
    x_mix, mix_gain, w_query, w_key, w_value, w_outgate, w_gates, gate_bias, gate_drift,
    head_gain, w_out, x_route, route_gain, routes, route_weight, w_gate_e, w_up_e, w_down_e,
):
    E = lax.axis_size("ep")
    TP = lax.axis_size("tp")
    rows, D = x_mix.shape
    width = w_query.shape[1]
    heads = width // HD
    NB = rows // BLK
    quarter = x_route.shape[0] // TP
    cap = 2 * quarter * TOPK // E
    H = TP // 2
    FH = w_gate_e.shape[2]
    MR = rows // TP
    anywhere = pl.BlockSpec(memory_space=pl.ANY)
    vmem = pl.BlockSpec(memory_space=pltpu.VMEM)
    V = pltpu.VMEM
    dma = pltpu.SemaphoreType.DMA
    SR = heads * HD + 16 * heads
    scratch = [
        V((rows, D), BF16), V((D, width), BF16), V((D, width), BF16), V((D, width), BF16), V((D, width), BF16),
        V((quarter, D), BF16), V((TP, D, FH), BF16), V((TP, D, FH), BF16), V((TP, FH, D), BF16),
        V((TP, width, D), BF16),
        V((E, cap, D), BF16), V((E, cap, D), BF16), V((TP, E * cap, FH), BF16),
        V((D // CHUNK, E // 2, cap, CHUNK), BF16), V((D // CHUNK, E // 2, cap, CHUNK), BF16),
        V((E // 2, cap, D), BF16), V((E // 2, cap, D), BF16),
        V((D // CHUNK, quarter, CHUNK), BF16), V((D // CHUNK, quarter, CHUNK), BF16),
        V((2 * TOPK, quarter), F32), V((2 * TOPK, quarter), F32),
        V((rows, width), BF16), V((rows, width), BF16), V((rows, width), BF16), V((rows, width), BF16),
        V((NB, 4 * heads, BLK), F32), V((NB, BLK, 4 * heads), F32), V((NB, 4 * heads, LANES), F32),
        V((NB, 2 * heads, HD, HD), F32), V((NB, 2 * heads, HD), F32),
        V((2, SR, HD), BF16), V((2, 8, LANES), F32), V((E, SR, HD), BF16), V((E, 8, LANES), F32),
        V((NB, 2 * heads, HD, HD), BF16), V((NB, 2 * heads, HD), F32), V((NB, 2 * heads, LANES), F32),
        V((rows, width), BF16), V((TP, MR, width), BF16), V((TOPK, quarter), jnp.int32), V((NB, 4 * heads, BLK), F32), V((4 * heads, D), BF16),
        dma((11,)), dma((1,)),
    ] + [dma((E,))] * 6 + [dma((TP,))] * 2 + [dma((5, H))] * 4 + [
        dma((D // CHUNK, E // 2)), dma((D // CHUNK, E // 2)), dma((E // 2,)), dma((E // 2,)),
        dma((D // CHUNK,)), dma((D // CHUNK,)), dma((1,)), dma((1,)),
    ]
    return pl.pallas_call(
        functools.partial(body, E, TP, heads, cap, quarter),
        out_shape=(jax.ShapeDtypeStruct((MR, D), BF16), jax.ShapeDtypeStruct((quarter, D), BF16)),
        in_specs=[anywhere] * 10 + [vmem] * 8,
        out_specs=(vmem, vmem),
        scratch_shapes=scratch,
        compiler_params=pltpu.CompilerParams(
            collective_id=0, has_side_effects=True, vmem_limit_bytes=67043328),
    )(
        x_mix, w_query, w_key, w_value, w_outgate, x_route, w_gate_e[0], w_up_e[0], w_down_e[0], w_out,
        mix_gain[None], route_gain[None], head_gain[None], w_gates.T, gate_bias.T, gate_drift[None], routes.T,
        route_weight.T,
    )


def solution(mesh):
    return jax.shard_map(
        shards,
        mesh=mesh,
        in_specs=(
            P("ep", None), P(), P(None, "tp"), P(None, "tp"), P(None, "tp"), P(None, "tp"), P(),
            P(None, "tp"), P("ep"), P("tp"), P("tp", None), P("ep", None), P(), P("ep", None),
            P(("ep", "tp"), None), P("ep", None, "tp"), P("ep", None, "tp"), P("ep", "tp", None),
        ),
        out_specs=(P(("ep", "tp"), None), P(("ep", "tp"), None)),
        check_vma=False,
    )
```
